32 devices in a mesh: sp: 4 (over y, x), tp: 8 (over z, core).
Axes of the slice: x: 2, y: 2, z: 4, core: 2. Of those that a mesh axis runs over, the one named last changes fastest.
Arguments:
- conv_value: bfloat16 [1024, 2048], P('tp', 'sp'), may hold values from -6 to 6
- conv_gate: bfloat16 [1024, 2048], P('tp', 'sp'), may hold values from -6 to 6
- conv_taps: float32 [1024, 31], P('tp'), may hold values from -2.2 to 2.2
- norm_gain: float32 [1024], replicated, may hold values from 0.1 to 1.9
- norm_bias: float32 [1024], replicated, may hold values from -3 to 3
- out_weight: bfloat16 [1024, 2048], replicated, may hold values from -0.1875 to 0.1875
- stream: bfloat16 [2048, 2048], P(('sp', 'tp')), may hold values from -6 to 6
- routes: int32 [2048, 2], P(('sp', 'tp')), may hold values from 0 to 3, all different within a row; in each aligned block of 64 rows (0 to 63, 64 to 127, ...) at most 32 rows name the same one
- route_weights: float32 [2048, 2], P(('sp', 'tp')), may hold values from 0.2 to 1
- expert_gain: float32 [2048], replicated, may hold values from 0.1 to 1.9
- expert_gate: bfloat16 [4, 2048, 7168], P('sp', None, 'tp'), may hold values from -0.125 to 0.125
- expert_up: bfloat16 [4, 2048, 7168], P('sp', None, 'tp'), may hold values from -0.125 to 0.125
- expert_down: bfloat16 [4, 7168, 2048], P('sp', 'tp'), may hold values from -0.0625 to 0.0625
Outputs:
- mixed: bfloat16 [2048, 2048], P(('sp', 'tp'))
The draws below stay inside these ranges and needn't reach their ends.
Inputs may be any that keep to these rules, and one draw needn't show every extreme that they name: `routes`: within each device's 64 rows every expert is named exactly 32 times; a row names distinct experts.
All inputs are finite; a program needn't handle non-finite values.
Results may differ from the reference program's by a relative error of at most 0.014.
Values may be sent and summed in bfloat16 or wider, within the bound.
A program may use at most 64 MiB of HBM per device.

```python
import math
import jax
import jax.numpy as jnp
import numpy as np
from jax import lax

D = 2048
CONV_CH = 1024
KERNEL = 31
FF_E = 7168
TOP = 2
TOK_DEV = 64
EXPERTS = 4
CAP = 32
TOKENS = 2048
N_TP = 8


def draw_conv_taps(key, part):
    base = jnp.clip(jax.random.normal(key, (CONV_CH, KERNEL), jnp.float32), -4.0, 4.0)
    scales = jnp.exp(jnp.linspace(math.log(0.5), math.log(3.0), CONV_CH))
    return (base * scales[:, None] * KERNEL ** (-0.5)).astype(jnp.float32)


def block_levels(stream_key, shape, pieces, low, high):
    factor_of, own = 1.0, jax.random.fold_in(stream_key, 6)
    for axis_at, shards_of in pieces:
        steps = jnp.exp(jax.random.uniform(jax.random.fold_in(own, axis_at), (shards_of,), jnp.float32, low / len(pieces), high / len(pieces)))
        factor_of = factor_of * jnp.repeat(steps, shape[axis_at] // shards_of).reshape([-1 if axis == axis_at else 1 for axis in range(len(shape))])
    return factor_of


def routed_block(stream_key, own, number, rows, count, top, bound, lean):
    ranking = jax.random.permutation(stream_key, count)
    heavy_load, usual = shares(count, rows * top, bound, lean, True), shares(count, rows * top, bound, lean, False)
    places = jnp.arange(count)

    def named(tallies, rotation):
        used = int((tallies > 0).sum())
        fixed = max(1, used // 4)
        moved = fixed + (places - fixed + rotation * (used - fixed)) % max(1, count - fixed)
        return jnp.zeros((count,), jnp.int32).at[ranking[jnp.where(places < fixed, places, moved)]].set(jnp.asarray(tallies, jnp.int32))

    tallies = jnp.where(number % 4 == 0, named(heavy_load, number // 4), named(usual, number - number // 4 - 1))
    mixed = jax.random.permutation(jax.random.fold_in(own, 3), count)
    donor, taker = mixed[0:count // 2 * 2:2], mixed[1:count // 2 * 2:2]
    margin = jnp.minimum(tallies[donor] - 1, bound - tallies[taker]) // 2
    margin = jnp.where((donor == ranking[0]) | (taker == ranking[0]) | (tallies[taker] == 0), 0, jnp.maximum(margin, 0))
    moved = jax.random.randint(jax.random.fold_in(own, 4), (count // 2,), 0, 1 << 20) % (margin + 1)
    tallies = tallies.at[donor].add(-moved).at[taker].add(moved)
    members = jnp.searchsorted(jnp.cumsum(tallies), jnp.arange(rows * top), side="right").astype(jnp.int32)
    listing = members.reshape(top, rows).T
    listing = listing[jax.random.permutation(jax.random.fold_in(own, 1), rows)]
    rotation = jax.random.randint(jax.random.fold_in(own, 2), (rows, 1), 0, top)
    return jnp.take_along_axis(listing, (jnp.arange(top)[None, :] + rotation) % top, axis=1)


def shares(number_of, total, bound, lean, full):
    loads = [(1 << 20) // math.isqrt(grade ** lean) + 1 for grade in range(1, number_of + 1)]
    largest = bound if full else min(bound, max(-(-total // number_of), total * loads[0] // sum(loads)))
    least = 1 if total - largest >= number_of - 1 else 0
    given, rest = [largest] + [least] * (number_of - 1), total - largest - least * (number_of - 1)
    while rest > 0:
        candidates = [i for i in range(1, number_of) if given[i] < largest] or [i for i in range(1, number_of) if given[i] < bound]
        pool, left = sum([loads[i] for i in candidates]), rest
        for i in candidates:
            extra = min(bound - given[i], max(1, left * loads[i] // pool), rest)
            given[i] = given[i] + extra
            rest = rest - extra
    return np.array(given)


def normal_values(own_key, shape, scale, limit, pieces=(), kind=jnp.bfloat16):
    drawn = scale * jax.random.normal(own_key, shape, jnp.float32)
    if pieces:
        drawn = drawn * block_levels(own_key, shape, pieces, -0.22, 0.18)
    return jnp.clip(drawn, -limit, limit).astype(kind)


def setup_inputs(seed: int = 0) -> dict:
    key_of = jax.random.split(jax.random.key(seed), 14)
    conv_value = normal_values(key_of[0], (CONV_CH, TOKENS), 1.0, 6.0, ((0, 8), (1, 4)))
    conv_gate = normal_values(key_of[1], (CONV_CH, TOKENS), 1.5, 6.0, ((0, 8), (1, 4)))
    conv_taps = draw_conv_taps(jax.random.fold_in(key_of[13], 71), 0)
    norm_gain = jnp.clip(1.0 + 0.18 * jax.random.normal(key_of[3], (CONV_CH,), jnp.float32), 0.1, 1.9)
    norm_bias = normal_values(key_of[4], (CONV_CH,), 0.5, 3.0, (), jnp.float32)
    out_weight = normal_values(key_of[5], (CONV_CH, D), CONV_CH ** -0.5, 0.1875)
    stream = normal_values(key_of[6], (TOKENS, D), 1.0, 6.0, ((0, 32),))
    routes_keys = jax.random.split(jax.random.fold_in(key_of[7], 1), TOKENS // TOK_DEV)
    routes_turns = jax.random.permutation(jax.random.fold_in(key_of[7], 3), TOKENS // TOK_DEV)
    routes = jax.vmap(lambda own, number: routed_block(jax.random.fold_in(key_of[7], 2), own, number, TOK_DEV, EXPERTS, TOP, CAP, 0))(routes_keys, routes_turns).reshape((TOKENS, TOP))
    route_weights = jnp.clip(0.2 + 0.8 * jax.random.uniform(key_of[8], (TOKENS, TOP), jnp.float32) ** block_levels(key_of[8], (TOKENS, TOP), ((0, 32),), -0.2, 0.2), 0.2, 1.0)
    expert_gain = jnp.clip(1.0 + 0.18 * jax.random.normal(key_of[9], (D,), jnp.float32), 0.1, 1.9)
    expert_gate = normal_values(key_of[10], (EXPERTS, D, FF_E), D ** -0.5, 0.125, ((0, 4), (2, 8)))
    expert_up = normal_values(key_of[11], (EXPERTS, D, FF_E), D ** -0.5, 0.125, ((0, 4), (2, 8)))
    expert_down = normal_values(key_of[12], (EXPERTS, FF_E, D), FF_E ** -0.5, 0.0625, ((0, 4), (1, 8)))
    return dict(conv_value=conv_value, conv_gate=conv_gate, conv_taps=conv_taps, norm_gain=norm_gain, norm_bias=norm_bias, out_weight=out_weight, stream=stream, routes=routes, route_weights=route_weights, expert_gain=expert_gain, expert_gate=expert_gate, expert_up=expert_up, expert_down=expert_down)


epsilon = 1e-06

def reference(conv_value, conv_gate, conv_taps, norm_gain, norm_bias, out_weight, stream, routes, route_weights, expert_gain, expert_gate, expert_up, expert_down):
    f32 = jnp.float32
    gated_input = (conv_value.astype(f32) * jax.nn.sigmoid(conv_gate.astype(f32))).astype(jnp.bfloat16)
    padded = jnp.pad(gated_input.astype(f32), ((0, 0), (KERNEL - 1, 0)))
    conv_sum = jnp.zeros((CONV_CH, TOKENS), f32)
    for offset in range(KERNEL):
        conv_sum = conv_sum + conv_taps[:, offset:offset + 1] * padded[:, offset:offset + TOKENS]
    conv_float = lax.optimization_barrier(conv_sum.astype(jnp.bfloat16)).astype(f32)
    center = lax.optimization_barrier(jnp.mean(conv_float, axis=0, keepdims=True))
    spread = lax.optimization_barrier(jnp.mean((conv_float - center) ** 2, axis=0, keepdims=True))
    scaled = (conv_float - center) * lax.rsqrt(spread + epsilon) * norm_gain[:, None] + norm_bias[:, None]
    activated = jax.nn.silu(scaled).astype(jnp.bfloat16)
    projected = lax.dot_general(activated, out_weight, (((0,), (0,)), ((), ())), preferred_element_type=f32)
    residual = (stream.astype(f32) + projected).astype(jnp.bfloat16)
    res_float = residual.astype(f32)
    normed = (res_float * lax.rsqrt(lax.optimization_barrier(jnp.mean(res_float * res_float, axis=1, keepdims=True)) + epsilon) * expert_gain).astype(jnp.bfloat16)
    blocks = TOKENS // TOK_DEV
    flat_ids = routes.reshape(blocks, TOK_DEV * TOP)
    onehot = (flat_ids[:, :, None] == jnp.arange(EXPERTS, dtype=jnp.int32)[None, None, :]).astype(jnp.int32)
    before = jnp.cumsum(onehot, axis=1) - onehot
    rank = lax.optimization_barrier(jnp.sum(before * onehot, axis=2))
    row_slot = jnp.arange(blocks, dtype=jnp.int32)[:, None] * CAP + rank
    token_of = (jnp.arange(blocks, dtype=jnp.int32)[:, None] * TOK_DEV + jnp.arange(TOK_DEV * TOP, dtype=jnp.int32)[None, :] // TOP).astype(jnp.int32)
    table = jnp.full((EXPERTS, blocks * CAP), TOKENS, jnp.int32).at[flat_ids, row_slot].set(token_of)
    weight_table = jnp.zeros((EXPERTS, blocks * CAP), f32).at[flat_ids, row_slot].set(route_weights.reshape(blocks, TOK_DEV * TOP))
    padded_rows = jnp.concatenate([normed, jnp.zeros((1, D), jnp.bfloat16)], axis=0)
    width_block = FF_E // N_TP

    def per_expert(total, inputs):
        index, weights, gate_w, up_w, down_w = inputs
        rows = padded_rows[index]
        gate_val = jnp.dot(rows, gate_w, preferred_element_type=f32)
        up_val = jnp.dot(rows, up_w, preferred_element_type=f32)
        hidden = (jax.nn.silu(gate_val) * up_val).astype(jnp.bfloat16)
        result = jnp.zeros((rows.shape[0], D), f32)
        for block in range(N_TP):
            part_sum = jnp.dot(hidden[:, block * width_block:(block + 1) * width_block], down_w[block * width_block:(block + 1) * width_block], preferred_element_type=f32)
            result = result + lax.optimization_barrier(part_sum.astype(jnp.bfloat16)).astype(f32)
        result = lax.optimization_barrier(result.astype(jnp.bfloat16)).astype(f32)
        return (total.at[index].add(weights[:, None] * result), None)
    start = jnp.zeros((TOKENS + 1, D), f32)
    total, unused = lax.scan(per_expert, start, (table, weight_table, expert_gate, expert_up, expert_down))
    return (res_float + total[:TOKENS]).astype(jnp.bfloat16)
```

```python
import functools

import jax
import jax.numpy as jnp
from jax import lax
from jax.experimental import pallas as pl
from jax.experimental.pallas import tpu as pltpu
from jax.sharding import PartitionSpec as P

epsilon = 1e-06
MESH = pl.DeviceIdType.MESH
QUARTERS = 4


def shifted(value, axis, steps):
    count = lax.axis_size(axis)
    initial, last = (max(0, -steps), min(count, count - steps))
    return lax.ppermute(value, axis, [(source, source + steps) for source in range(initial, last)])


def moe_kernel(
    S,
    Z,
    C,
    packed,
    normed_ref,
    resid_ref,
    routes_ref,
    weights_ref,
    gate_hbm,
    up_hbm,
    down_hbm,
    out_ref,
    sendbuf,
    xbuf,
    wg,
    wu,
    wd,
    hid,
    mine,
    pout,
    pin,
    rbuf,
    fin,
    ret,
    w_sem,
    disp_send,
    disp_recv,
    agz_send,
    agz_recv,
    ags_send,
    ags_recv,
    rss_send,
    rss_recv,
    rsz_send,
    rsz_recv,
    ret_send,
    ret_recv,
):
    f32, bf16 = jnp.float32, jnp.bfloat16
    s_me = lax.axis_index("sp")
    t_me = lax.axis_index("tp")
    z_me, c_me = t_me // 2, t_me % 2
    half = Z // 2
    Q = S // QUARTERS
    W = normed_ref.shape[1]
    tokens = normed_ref.shape[0]
    F = down_hbm.shape[1]
    QR = Q * C
    M = Z * 2 * QR

    def sp_peer(steps):
        return (lax.rem(s_me + steps + S, S), t_me)

    def z_peer(steps):
        return (s_me, lax.rem(z_me + steps + Z, Z) * 2 + c_me)

    sibling = (s_me, z_me * 2 + 1 - c_me)

    loads = []
    if packed:
        tiles = F // 128
        for j in range(tiles):
            for k, src in enumerate((gate_hbm, up_hbm)):
                loads.append(
                    pltpu.make_async_copy(
                        src.at[0, :, pl.ds(j * 128, 128)],
                        wg.at[j, :, pl.ds(k * 128, 128)],
                        w_sem.at[2 * j + k],
                    )
                )
    else:
        tiles = 1
        loads.append(pltpu.make_async_copy(gate_hbm.at[0], wg.at[0], w_sem.at[0]))
        loads.append(pltpu.make_async_copy(up_hbm.at[0], wu.at[0], w_sem.at[1]))
    down_load = pltpu.make_async_copy(down_hbm.at[0], wd, w_sem.at[2 * tiles])
    for cp in loads:
        cp.start()
    down_load.start()

    barrier = pltpu.get_barrier_semaphore()
    peers = [sp_peer(j) for j in range(1, S)] + [z_peer(1), z_peer(-1), sibling]
    for peer in peers:
        pl.semaphore_signal(barrier, inc=1, device_id=peer, device_id_type=MESH)

    r0, r1 = routes_ref[0:1, :], routes_ref[1:2, :]
    w0, w1 = weights_ref[0:1, :], weights_ref[1:2, :]
    ids = s_me - lax.broadcasted_iota(jnp.int32, (S, tokens), 0)
    ids = jnp.where(ids < 0, ids + S, ids)
    hit0, hit1 = r0 == ids, r1 == ids
    named = jnp.where(hit0 | hit1, 1.0, 0.0)
    row_w = jnp.where(hit0, w0, 0.0) + jnp.where(hit1, w1, 0.0)
    earlier = jnp.where(
        lax.broadcasted_iota(jnp.int32, (tokens, tokens), 0)
        < lax.broadcasted_iota(jnp.int32, (tokens, tokens), 1),
        1.0,
        0.0,
    )
    rank = jnp.dot(named.astype(bf16), earlier.astype(bf16), preferred_element_type=f32)
    slot = lax.broadcasted_iota(jnp.int32, (C, tokens), 0).astype(f32)
    choose, weigh = [], []
    for j in range(S):
        pick = jnp.where(rank[j : j + 1, :] == slot, named[j : j + 1, :], 0.0)
        choose.append(pick)
        weigh.append(pick * row_w[j : j + 1, :])
    rows = normed_ref[...]
    sent = jnp.dot(
        jnp.concatenate(choose, axis=0).astype(bf16), rows, preferred_element_type=f32
    ).astype(bf16)
    xbuf[0, 0, 0, 0] = sent[0:C]
    for j in range(1, S):
        sendbuf[j] = sent[j * C : (j + 1) * C]

    pl.semaphore_wait(barrier, len(peers))

    sends = []

    def remote(src, dst, send_sem, recv_sem, peer):
        return pltpu.make_async_remote_copy(
            src_ref=src,
            dst_ref=dst,
            send_sem=send_sem,
            recv_sem=recv_sem,
            device_id=peer,
            device_id_type=MESH,
        )

    def start(cp):
        cp.start()
        sends.append(cp)

    def disp(j):
        return remote(
            sendbuf.at[j],
            xbuf.at[j // Q, 0, 0, j % Q],
            disp_send.at[j],
            disp_recv.at[j],
            sp_peer(-j),
        )

    def sign(d):
        return 1 if d == 0 else -1

    def reach(d, q):
        return half if d == q % 2 else half - 1

    def agz(d, k, q):
        return remote(
            xbuf.at[q, (-sign(d) * (k - 1)) % Z, 0],
            xbuf.at[q, (-sign(d) * k) % Z, 0],
            agz_send.at[d, k - 1, q],
            agz_recv.at[d, k - 1, q],
            z_peer(sign(d)),
        )

    def ags(q, r):
        return remote(
            xbuf.at[q, r, 0], xbuf.at[q, r, 1], ags_send.at[q, r], ags_recv.at[q, r], sibling
        )

    def rss(q, r):
        return remote(
            pout.at[q, r], pin.at[q, r], rss_send.at[q, r], rss_recv.at[q, r], sibling
        )

    def rsz(d, k, q):
        return remote(
            mine.at[q, (sign(d) * k) % Z],
            rbuf.at[d, k - 1, q],
            rsz_send.at[d, k - 1, q],
            rsz_recv.at[d, k - 1, q],
            z_peer(sign(d)),
        )

    def back(j):
        return remote(
            fin.at[j // Q, j % Q], ret.at[j], ret_send.at[j], ret_recv.at[j], sp_peer(j)
        )

    def first_hop(q):
        for i in range(Q):
            j = q * Q + i
            if j > 0:
                disp(j).wait_recv()
        for d in (q % 2, 1 - q % 2):
            if reach(d, q) >= 1:
                start(agz(d, 1, q))
        start(ags(q, 0))

    def forward(q, k):
        for d in (q % 2, 1 - q % 2):
            if reach(d, q) >= k:
                agz(d, k, q).wait_recv()
                if k < reach(d, q):
                    start(agz(d, k + 1, q))
                start(ags(q, (-sign(d) * k) % Z))

    def ready(q):
        for r in range(Z):
            ags(q, r).wait_recv()

    def ffn_up(q):
        if q == 0:
            for cp in loads:
                cp.wait()

        def tile(j, carry):
            x = xbuf[q].reshape(M, W)
            if packed:
                both = jnp.dot(x, wg[j], preferred_element_type=f32)
                g, u = both[:, :128], both[:, 128:]
                hid[:, pl.ds(pl.multiple_of(j * 128, 128), 128)] = (jax.nn.silu(g) * u).astype(bf16)
            else:
                g = jnp.dot(x, wg[0], preferred_element_type=f32)
                u = jnp.dot(x, wu[0], preferred_element_type=f32)
                hid[...] = (jax.nn.silu(g) * u).astype(bf16)
            return carry

        lax.fori_loop(0, tiles, tile, 0, unroll=True)

    step = 512

    def ffn_down(q):
        if q == 0:
            down_load.wait()

        def tile(n, carry):
            cols = pl.ds(pl.multiple_of(n * step, step), step)
            y = jnp.dot(hid[...], wd[:, cols], preferred_element_type=f32).astype(bf16)
            y = y.reshape(Z, 2, QR, step)
            mine[q, :, :, cols] = y[:, 0]
            pout[q, :, :, cols] = y[:, 1]
            return carry

        lax.fori_loop(0, W // step, tile, 0, unroll=True)
        for k in range(half, 0, -1):
            for r in sorted({k % Z, -k % Z}):
                start(rss(q, r))
        start(rss(q, 0))

    def pair_sum(q, r, extra=None):
        rss(q, r).wait_recv()
        total = mine[q, r].astype(f32) + pin[q, r].astype(f32)
        if extra is not None:
            total = total + extra[...].astype(f32)
        mine[q, r] = total.astype(bf16)

    def launch(q):
        for k in range(half, 0, -1):
            for d in (q % 2, 1 - q % 2):
                if reach(d, q) == k:
                    pair_sum(q, (sign(d) * k) % Z)
                    start(rsz(d, k, q))

    def relay(q):
        for k in range(half - 1, 0, -1):
            for d in (q % 2, 1 - q % 2):
                if reach(d, q) > k:
                    rsz(d, k + 1, q).wait_recv()
                    pair_sum(q, (sign(d) * k) % Z, rbuf.at[d, k, q])
                    start(rsz(d, k, q))

    def finish(q):
        rss(q, 0).wait_recv()
        total = mine[q, 0].astype(f32) + pin[q, 0].astype(f32)
        for d in (0, 1):
            if reach(d, q) >= 1:
                rsz(d, 1, q).wait_recv()
                total = total + rbuf[d, 0, q].astype(f32)
        done = total.astype(bf16).reshape(Q, C, W)
        if q == 0:
            ret[0] = done[0]
        fin[q] = done
        for i in range(Q):
            j = q * Q + i
            if j > 0:
                start(back(j))

    def far(f, q):
        for k in range(2, half + 1):
            f(q, k)

    for j in range(1, S):
        start(disp(j))
    first_hop(0)
    first_hop(1)
    forward(0, 1)
    first_hop(2)
    forward(1, 1)
    first_hop(3)
    far(forward, 0)
    ready(0)
    ffn_up(0)
    forward(2, 1)
    far(forward, 1)
    ffn_down(0)
    forward(3, 1)
    ready(1)
    launch(0)
    ffn_up(1)
    far(forward, 2)
    ffn_down(1)
    relay(0)
    far(forward, 3)
    ready(2)
    launch(1)
    ffn_up(2)
    ffn_down(2)
    relay(1)
    ready(3)
    launch(2)
    ffn_up(3)
    finish(0)
    ffn_down(3)
    relay(2)
    launch(3)
    finish(1)
    relay(3)
    finish(2)
    finish(3)

    spread = jnp.concatenate(weigh, axis=0).T
    high = spread.astype(bf16)
    low = (spread - high.astype(f32)).astype(bf16)
    for j in range(1, S):
        back(j).wait_recv()
    got = ret[...].reshape(S * C, W)
    mix = jnp.dot(high, got, preferred_element_type=f32) + jnp.dot(
        low, got, preferred_element_type=f32
    )
    out_ref[...] = (resid_ref[...].astype(f32) + mix).astype(bf16)
    for cp in sends:
        cp.wait_send()


def routed_experts(normed, residual, routes, route_weights, gate_w, up_w, down_w):
    S, T = lax.axis_size("sp"), lax.axis_size("tp")
    Z, half = T // 2, T // 4
    tokens, W = normed.shape
    C = routes.shape[1] * tokens // S
    Q = S // QUARTERS
    F = gate_w.shape[2]
    packed = F % 128 == 0
    tiles = F // 128 if packed else 1
    M = Z * 2 * Q * C
    bf16 = jnp.bfloat16
    vmem = pl.BlockSpec(memory_space=pltpu.VMEM)
    hbm = pl.BlockSpec(memory_space=pl.ANY)
    dma = pltpu.SemaphoreType.DMA
    quarter = (Q * C, W)
    return pl.pallas_call(
        functools.partial(moe_kernel, S, Z, C, packed),
        out_shape=jax.ShapeDtypeStruct((tokens, W), bf16),
        in_specs=[vmem] * 4 + [hbm] * 3,
        out_specs=vmem,
        scratch_shapes=[
            pltpu.VMEM((S, C, W), bf16),
            pltpu.VMEM((QUARTERS, Z, 2, Q, C, W), bf16),
            pltpu.VMEM((tiles, W, 256) if packed else (1, W, F), bf16),
            pltpu.VMEM((1, 16, 128) if packed else (1, W, F), bf16),
            pltpu.VMEM((F, W), bf16),
            pltpu.VMEM((M, F), bf16),
            pltpu.VMEM((QUARTERS, Z) + quarter, bf16),
            pltpu.VMEM((QUARTERS, Z) + quarter, bf16),
            pltpu.VMEM((QUARTERS, Z) + quarter, bf16),
            pltpu.VMEM((2, half, QUARTERS) + quarter, bf16),
            pltpu.VMEM((QUARTERS, Q, C, W), bf16),
            pltpu.VMEM((S, C, W), bf16),
            dma((2 * tiles + 1,)),
            dma((S,)),
            dma((S,)),
            dma((2, half, QUARTERS)),
            dma((2, half, QUARTERS)),
            dma((QUARTERS, Z)),
            dma((QUARTERS, Z)),
            dma((QUARTERS, Z)),
            dma((QUARTERS, Z)),
            dma((2, half, QUARTERS)),
            dma((2, half, QUARTERS)),
            dma((S,)),
            dma((S,)),
        ],
        compiler_params=pltpu.CompilerParams(
            collective_id=0, has_side_effects=True, vmem_limit_bytes=56 * 1024 * 1024
        ),
        name="routed_experts",
    )(normed, residual, routes.T, route_weights.T, gate_w, up_w, down_w)


def exchange_kernel(T, blocks_ref, out_ref, land, send_sem, recv_sem):
    s_me = lax.axis_index("sp")
    t_me = lax.axis_index("tp")
    barrier = pltpu.get_barrier_semaphore()
    for i in range(1, T):
        peer = (s_me, lax.rem(t_me + i, T))
        pl.semaphore_signal(barrier, inc=1, device_id=peer, device_id_type=MESH)
    pl.semaphore_wait(barrier, T - 1)
    copies = []
    for i in range(1, T):
        target = lax.rem(t_me + i, T)
        copies.append(
            pltpu.make_async_remote_copy(
                src_ref=blocks_ref.at[target],
                dst_ref=land.at[t_me],
                send_sem=send_sem.at[i],
                recv_sem=recv_sem.at[i],
                device_id=(s_me, target),
                device_id_type=MESH,
            )
        )
    for cp in copies:
        cp.start()
    land[t_me] = blocks_ref[t_me]
    for cp in copies:
        cp.wait()
    out_ref[...] = land[...]


def exchange(blocks):
    T = blocks.shape[0]
    vmem = pl.BlockSpec(memory_space=pltpu.VMEM)
    return pl.pallas_call(
        functools.partial(exchange_kernel, T),
        out_shape=jax.ShapeDtypeStruct(blocks.shape, blocks.dtype),
        in_specs=[vmem],
        out_specs=vmem,
        scratch_shapes=[
            pltpu.VMEM(blocks.shape, blocks.dtype),
            pltpu.SemaphoreType.DMA((T,)),
            pltpu.SemaphoreType.DMA((T,)),
        ],
        compiler_params=pltpu.CompilerParams(collective_id=1, has_side_effects=True),
        name="exchange",
    )(blocks)


class Link:
    def __init__(self):
        self.sent = []

    def copy(self, src, dst, send_sem, recv_sem, peer):
        return pltpu.make_async_remote_copy(
            src_ref=src,
            dst_ref=dst,
            send_sem=send_sem,
            recv_sem=recv_sem,
            device_id=peer,
            device_id_type=MESH,
        )

    def start(self, cp, cond=None):
        self.sent.append((cp, cond))
        if cond is None:
            cp.start()
        else:
            pl.when(cond)(cp.start)

    def drain(self):
        for cp, cond in self.sent:
            if cond is None:
                cp.wait_send()
            else:
                pl.when(cond)(cp.wait_send)


def fused_kernel(
    T,
    C,
    taps_n,
    value_ref,
    vgate_ref,
    taps_ref,
    gain_ref,
    bias_ref,
    routes_ref,
    weights_ref,
    egain_ref,
    stream_ref,
    outw_hbm,
    gate_hbm,
    up_hbm,
    down_hbm,
    out_ref,
    gbuf,
    halo_out,
    halo_in,
    cbuf,
    land,
    outw,
    res,
    meta,
    cho,
    hi,
    lo,
    tok,
    sbuf,
    X,
    wg,
    wd,
    hid,
    mine,
    pout,
    pin,
    ret,
    tot,
    tout,
    tin,
    w_sem,
    halo_sem,
    ex_send,
    ex_recv,
    meta_send,
    meta_recv,
    tz_send,
    tz_recv,
    pl_send,
    pl_recv,
    sx_send,
    sx_recv,
    sy_send,
    sy_recv,
    rt_send,
    rt_recv,
    zo_send,
    zo_recv,
):
    f32, bf16 = jnp.float32, jnp.bfloat16
    s = lax.axis_index("sp")
    t = lax.axis_index("tp")
    z, c = t // 2, t % 2
    Z, J = T // 2, 4
    gy, gx = s // 2, s % 2
    W = out_ref.shape[1]
    tokens = out_ref.shape[0]
    F = wd.shape[0]
    tiles = F // 128
    ch, run = value_ref.shape
    rim = gbuf.shape[0] - run
    link = Link()

    def plane(j):
        return (lax.rem(gy + j // 2, 2) * 2 + lax.rem(gx + j % 2, 2), t)

    def at_z(zt):
        return (s, zt * 2 + c)

    sibling = (s, z * 2 + 1 - c)

    zp = [z, 1 + z % 2, 2 + z // 2 - 2 * (z % 2), 3 - 3 * (z // 2)]

    outw_load = pltpu.make_async_copy(outw_hbm, outw, w_sem.at[2 * tiles + 1])
    outw_load.start()
    loads = []
    for j in range(tiles):
        for k, src in enumerate((gate_hbm, up_hbm)):
            loads.append(
                pltpu.make_async_copy(
                    src.at[0, :, pl.ds(j * 128, 128)],
                    wg.at[j, :, pl.ds(k * 128, 128)],
                    w_sem.at[2 * j + k],
                )
            )
    down_load = pltpu.make_async_copy(down_hbm.at[0], wd, w_sem.at[2 * tiles])
    for cp in loads:
        cp.start()
    down_load.start()

    barrier = pltpu.get_barrier_semaphore()
    peers = [plane(j) for j in range(1, J)] + [(s, lax.rem(t + i, T)) for i in range(1, T)]
    for peer in peers:
        pl.semaphore_signal(barrier, inc=1, device_id=peer, device_id_type=MESH)

    gated = (
        value_ref[...].astype(f32) * jax.nn.sigmoid(vgate_ref[...].astype(f32))
    ).astype(bf16)
    turned = gated.astype(f32).T
    gbuf[rim:, :] = turned
    halo_out[...] = turned[run - rim :, :].astype(bf16)
    meta[z, 0:2, 0:tokens] = routes_ref[...].astype(f32)
    meta[z, 2:4, 0:tokens] = weights_ref[...]

    pl.semaphore_wait(barrier, len(peers))

    S = J
    halo = link.copy(
        halo_out, halo_in, halo_sem.at[0], halo_sem.at[1], (lax.rem(s + 1, S), t)
    )
    link.start(halo, s < S - 1)

    def mz(i, zs):
        return link.copy(
            meta.at[z], meta.at[z], meta_send.at[i - 1], meta_recv.at[z], at_z(zs)
        )

    for i in range(1, Z):
        link.start(mz(i, lax.rem(z + i, Z)))

    def conv(b):
        acc = jnp.zeros((tokens, ch), f32)
        for j in range(taps_n):
            lead = rim - (taps_n - 1) + b * tokens + j
            acc = acc + taps_ref[j : j + 1, :] * gbuf[lead : lead + tokens, :]
        cbuf[b] = acc.astype(bf16)

    for b in range(1, T):
        conv(b)

    @pl.when(s > 0)
    def _():
        halo.wait_recv()
        gbuf[0:rim, :] = halo_in[...].astype(f32)

    @pl.when(s == 0)
    def _():
        gbuf[0:rim, :] = jnp.zeros((rim, ch), f32)

    conv(0)

    exchanges = []
    for i in range(1, T):
        target = lax.rem(t + i, T)
        cp = link.copy(
            cbuf.at[target], land.at[t], ex_send.at[i - 1], ex_recv.at[i - 1], (s, target)
        )
        link.start(cp)
        exchanges.append(cp)
    land[t] = cbuf[t]

    for i in range(1, Z):
        zs = lax.rem(z + Z - i, Z)
        link.copy(
            meta.at[zs], meta.at[zs], meta_send.at[i - 1], meta_recv.at[zs], at_z(zs)
        ).wait_recv()

    row = lax.broadcasted_iota(jnp.int32, (J, tokens), 0)
    ids = (((gy + (row >> 1)) & 1) * 2 + ((gx + (row & 1)) & 1)).astype(f32)
    earlier = jnp.where(
        lax.broadcasted_iota(jnp.int32, (tokens, tokens), 0)
        < lax.broadcasted_iota(jnp.int32, (tokens, tokens), 1),
        1.0,
        0.0,
    ).astype(bf16)
    slot = lax.broadcasted_iota(jnp.int32, (C, tokens), 0).astype(f32)
    for p in range(Z):
        m = meta[zp[p]]
        r0, r1 = m[0:1, :tokens], m[1:2, :tokens]
        w0, w1 = m[2:3, :tokens], m[3:4, :tokens]
        hit0, hit1 = r0 == ids, r1 == ids
        named = jnp.where(hit0 | hit1, 1.0, 0.0)
        row_w = jnp.where(hit0, w0, 0.0) + jnp.where(hit1, w1, 0.0)
        rank = jnp.dot(named.astype(bf16), earlier, preferred_element_type=f32)
        choose, weigh = [], []
        for j in range(J):
            pick = jnp.where(rank[j : j + 1, :] == slot, named[j : j + 1, :], 0.0)
            choose.append(pick)
            weigh.append(pick * row_w[j : j + 1, :])
        cho[p] = jnp.concatenate(choose, axis=0).astype(bf16)
        spread = jnp.concatenate(weigh, axis=0).T
        high = spread.astype(bf16)
        hi[p] = high
        lo[p] = (spread - high.astype(f32)).astype(bf16)

    for cp in exchanges:
        cp.wait_recv()
    whole = jnp.concatenate([land[i] for i in range(T)], axis=1).astype(f32)
    center = jnp.mean(whole, axis=1, keepdims=True)
    whole = whole - center
    var = jnp.mean(whole * whole, axis=1, keepdims=True)
    act = jax.nn.silu(
        whole * lax.rsqrt(var + epsilon) * gain_ref[...] + bias_ref[...]
    ).astype(bf16)
    outw_load.wait()
    step = 512
    square = jnp.zeros((tokens, 1), f32)
    for n in range(W // step):
        cut = slice(n * step, (n + 1) * step)
        r = (
            stream_ref[:, cut].astype(f32)
            + jnp.dot(act, outw[:, cut], preferred_element_type=f32)
        ).astype(bf16)
        res[:, cut] = r
        rf = r.astype(f32)
        square = square + jnp.sum(rf * rf, axis=1, keepdims=True)
    scale = lax.rsqrt(square * (1.0 / W) + epsilon)
    for n in range(W // step):
        cut = slice(n * step, (n + 1) * step)
        tok[z, :, cut] = (res[:, cut].astype(f32) * scale * egain_ref[:, cut]).astype(bf16)

    def sign(d):
        return 1 if d == 0 else -1

    def inside(v):
        return (v >= 0) & (v < Z)

    def tz(d, k):
        block = lax.rem(z - sign(d) * (k - 1) + Z, Z)
        return link.copy(
            tok.at[block],
            tok.at[block],
            tz_send.at[d, k - 1],
            tz_recv.at[d, k - 1],
            at_z(lax.rem(z + sign(d) + Z, Z)),
        )

    def tz_in(d, k):
        block = lax.rem(z - sign(d) * k + Z, Z)
        return link.copy(
            tok.at[block],
            tok.at[block],
            tz_send.at[d, k - 1],
            tz_recv.at[d, k - 1],
            at_z(lax.rem(z + sign(d) + Z, Z)),
        )

    def arrive(k):
        for d in (0, 1):
            sg = sign(d)
            pl.when(inside(z - sg * k))(tz_in(d, k).wait_recv)
            if k < Z - 1:
                link.start(tz(d, k + 1), inside(z - sg * k) & inside(z + sg))

    def pland(p, j):
        return link.copy(
            sbuf.at[p, j - 1], X.at[p, j, 0], pl_send.at[p, j - 1], pl_recv.at[p, j - 1], plane(j)
        )

    def sibx(p, j):
        return link.copy(X.at[p, j, 0], X.at[p, j, 1], sx_send.at[p, j], sx_recv.at[p, j], sibling)

    def select(p):
        for n in range(W // step):
            cut = slice(n * step, (n + 1) * step)
            sel = jnp.dot(cho[p], tok[zp[p], :, cut], preferred_element_type=f32).astype(bf16)
            X[p, 0, 0, :, cut] = sel[0:C]
            for j in range(1, J):
                sbuf[p, j - 1, :, cut] = sel[j * C : (j + 1) * C]
        for j in (3, 1, 2):
            link.start(pland(p, j))
        link.start(sibx(p, 0))

    def gather(p):
        for j in (3, 1, 2):
            pland(p, j).wait_recv()
            link.start(sibx(p, j))
        for j in range(J):
            sibx(p, j).wait_recv()

    M = J * 2 * C

    def ffn_up(p):
        if p == 0:
            for cp in loads:
                cp.wait()
        for j in range(tiles):
            x = X[p].reshape(M, W)
            both = jnp.dot(x, wg[j], preferred_element_type=f32)
            g, u = both[:, :128], both[:, 128:]
            hid[:, j * 128 : (j + 1) * 128] = (jax.nn.silu(g) * u).astype(bf16)

    H = pout.shape[0]
    span = W // H

    def siby(p, h):
        return link.copy(
            pout.at[h, p], pin.at[h, p], sy_send.at[p, h], sy_recv.at[p, h], sibling
        )

    def ffn_down(p):
        if p == 0:
            down_load.wait()
        for h in range(H):
            for n in range(span // step):
                cut = slice(n * step, (n + 1) * step)
                full = slice(h * span + n * step, h * span + (n + 1) * step)
                y = jnp.dot(hid[...], wd[:, full], preferred_element_type=f32).astype(bf16)
                y = y.reshape(J, 2, C, step)
                mine[h, p, :, :, cut] = y[:, 0]
                pout[h, p, :, :, cut] = y[:, 1]
            link.start(siby(p, h))

    def back(p, j, h):
        return link.copy(
            mine.at[h, p, j],
            ret.at[h, p, j],
            rt_send.at[p, j - 1, h],
            rt_recv.at[p, j - 1, h],
            plane(j),
        )

    def give(p):
        for h in range(H):
            siby(p, h).wait_recv()
            for j in range(J):
                total = (mine[h, p, j].astype(f32) + pin[h, p, j].astype(f32)).astype(bf16)
                if j == 0:
                    ret[h, p, 0] = total
                else:
                    mine[h, p, j] = total
            for j in (3, 1, 2):
                link.start(back(p, j, h))

    def zout(p, h):
        return link.copy(
            tout.at[h, p - 1], tin.at[h, z], zo_send.at[p - 1, h], zo_recv.at[z, h], at_z(zp[p])
        )

    def zin(p, h):
        return link.copy(
            tout.at[h, p - 1],
            tin.at[h, zp[p]],
            zo_send.at[p - 1, h],
            zo_recv.at[zp[p], h],
            at_z(zp[p]),
        )

    def mixed_part(p, h):
        for j in (3, 1, 2):
            back(p, j, h).wait_recv()
        got = ret[h, p].reshape(J * C, span)
        return jnp.dot(hi[p], got, preferred_element_type=f32) + jnp.dot(
            lo[p], got, preferred_element_type=f32
        )

    def combine(p):
        for h in range(H):
            tout[h, p - 1] = mixed_part(p, h).astype(bf16)
            link.start(zout(p, h))

    for d in (0, 1):
        link.start(tz(d, 1), inside(z + sign(d)))
    select(0)
    arrive(1)
    select(1)
    gather(0)
    ffn_up(0)
    ffn_down(0)
    arrive(2)
    select(2)
    gather(1)
    ffn_up(1)
    ffn_down(1)
    arrive(3)
    select(3)
    give(1)
    gather(2)
    ffn_up(2)
    ffn_down(2)
    gather(3)
    ffn_up(3)
    ffn_down(3)
    give(3)
    give(2)
    give(0)
    combine(1)
    combine(3)
    combine(2)
    for h in range(H):
        cut = slice(h * span, (h + 1) * span)
        tot[:, cut] = res[:, cut].astype(f32) + mixed_part(0, h)
    for h in range(H):
        cut = slice(h * span, (h + 1) * span)
        acc = tot[:, cut]
        for p in range(1, Z):
            zin(p, h).wait_recv()
            acc = acc + tin[h, zp[p]].astype(f32)
        out_ref[:, cut] = acc.astype(bf16)
    link.drain()


def fused(
    conv_value, conv_gate, conv_taps, norm_gain, norm_bias, out_weight, stream,
    routes, route_weights, expert_gain, gate_w, up_w, down_w,
):
    T = lax.axis_size("tp")
    S, Z = lax.axis_size("sp"), T // 2
    tokens, W = stream.shape
    C = routes.shape[1] * tokens // S
    F = gate_w.shape[2]
    ch, run = conv_value.shape
    taps_n = conv_taps.shape[1]
    rim = -(-(taps_n - 1) // 16) * 16
    tiles = F // 128
    H = 2
    span = W // H
    f32, bf16 = jnp.float32, jnp.bfloat16
    vmem = pl.BlockSpec(memory_space=pltpu.VMEM)
    hbm = pl.BlockSpec(memory_space=pl.ANY)
    dma = pltpu.SemaphoreType.DMA
    rows = (H, Z, S, C, span)
    return pl.pallas_call(
        functools.partial(fused_kernel, T, C, taps_n),
        out_shape=jax.ShapeDtypeStruct((tokens, W), bf16),
        in_specs=[vmem] * 9 + [hbm] * 4,
        out_specs=vmem,
        scratch_shapes=[
            pltpu.VMEM((rim + run, ch), f32),
            pltpu.VMEM((rim, ch), bf16),
            pltpu.VMEM((rim, ch), bf16),
            pltpu.VMEM((T, tokens, ch), bf16),
            pltpu.VMEM((T, tokens, ch), bf16),
            pltpu.VMEM(out_weight.shape, bf16),
            pltpu.VMEM((tokens, W), bf16),
            pltpu.VMEM((Z, 8, 128), f32),
            pltpu.VMEM((Z, S * C, tokens), bf16),
            pltpu.VMEM((Z, tokens, S * C), bf16),
            pltpu.VMEM((Z, tokens, S * C), bf16),
            pltpu.VMEM((Z, tokens, W), bf16),
            pltpu.VMEM((Z, S - 1, C, W), bf16),
            pltpu.VMEM((Z, S, 2, C, W), bf16),
            pltpu.VMEM((tiles, W, 256), bf16),
            pltpu.VMEM((F, W), bf16),
            pltpu.VMEM((S * 2 * C, F), bf16),
            pltpu.VMEM(rows, bf16),
            pltpu.VMEM(rows, bf16),
            pltpu.VMEM(rows, bf16),
            pltpu.VMEM(rows, bf16),
            pltpu.VMEM((tokens, W), f32),
            pltpu.VMEM((H, Z - 1, tokens, span), bf16),
            pltpu.VMEM((H, Z, tokens, span), bf16),
            dma((2 * tiles + 2,)),
            dma((2,)),
            dma((T - 1,)),
            dma((T - 1,)),
            dma((Z - 1,)),
            dma((Z,)),
            dma((2, Z - 1)),
            dma((2, Z - 1)),
            dma((Z, S - 1)),
            dma((Z, S - 1)),
            dma((Z, S)),
            dma((Z, S)),
            dma((Z, H)),
            dma((Z, H)),
            dma((Z, S - 1, H)),
            dma((Z, S - 1, H)),
            dma((Z - 1, H)),
            dma((Z, H)),
        ],
        compiler_params=pltpu.CompilerParams(
            collective_id=2, has_side_effects=True, vmem_limit_bytes=60 * 1024 * 1024
        ),
        name="fused_block",
    )(
        conv_value, conv_gate, conv_taps.T, norm_gain.reshape(1, -1), norm_bias.reshape(1, -1),
        routes.T, route_weights.T, expert_gain.reshape(1, -1), stream,
        out_weight, gate_w, up_w, down_w,
    )


def per_device(
    conv_value,
    conv_gate,
    conv_taps,
    norm_gain,
    norm_bias,
    out_weight,
    stream,
    routes,
    route_weights,
    expert_gain,
    expert_gate,
    expert_up,
    expert_down,
):
    square_plane = lax.axis_size("sp") == 4 and lax.axis_size("tp") == 8
    if square_plane and expert_gate.shape[2] % 128 == 0 and conv_value.shape[0] % 128 == 0:
        return fused(
            conv_value, conv_gate, conv_taps, norm_gain, norm_bias, out_weight, stream,
            routes, route_weights, expert_gain, expert_gate, expert_up, expert_down,
        )
    f32 = jnp.float32
    local_ch = conv_value.shape[0]
    run_len = conv_value.shape[1]
    kernel_len = conv_taps.shape[1]
    gated_input = (conv_value.astype(f32) * jax.nn.sigmoid(conv_gate.astype(f32))).astype(
        jnp.bfloat16
    )
    left_rim = shifted(gated_input[:, run_len - (kernel_len - 1) :], "sp", 1)
    padded = jnp.concatenate([left_rim, gated_input], axis=1).astype(f32)
    conv_sum = jnp.zeros((local_ch, run_len), f32)
    for offset in range(kernel_len):
        conv_sum = (
            conv_sum + conv_taps[:, offset : offset + 1] * padded[:, offset : offset + run_len]
        )
    conv_out = conv_sum.astype(jnp.bfloat16)
    parts = lax.axis_size("tp")
    tok_rows = run_len // parts
    pieces = exchange(conv_out.T.reshape(parts, tok_rows, local_ch))
    whole_conv = pieces.transpose(1, 0, 2).reshape(tok_rows, parts * local_ch).astype(f32)
    center = jnp.mean(whole_conv, axis=1, keepdims=True)
    spread = jnp.mean((whole_conv - center) ** 2, axis=1, keepdims=True)
    scaled = (whole_conv - center) * lax.rsqrt(spread + epsilon) * norm_gain + norm_bias
    token_major = jax.nn.silu(scaled).astype(jnp.bfloat16)
    projected = jnp.dot(token_major, out_weight, preferred_element_type=f32)
    residual = (stream.astype(f32) + projected).astype(jnp.bfloat16)
    res_float = residual.astype(f32)
    normed = (
        res_float
        * lax.rsqrt(jnp.mean(res_float * res_float, axis=1, keepdims=True) + epsilon)
        * expert_gain
    ).astype(jnp.bfloat16)
    return routed_experts(
        normed, residual, routes, route_weights, expert_gate, expert_up, expert_down
    )


def solution(mesh):
    return jax.shard_map(
        per_device,
        mesh=mesh,
        in_specs=(
            P("tp", "sp"),
            P("tp", "sp"),
            P("tp", None),
            P(),
            P(),
            P(),
            P(("sp", "tp"), None),
            P(("sp", "tp"), None),
            P(("sp", "tp"), None),
            P(),
            P("sp", None, "tp"),
            P("sp", None, "tp"),
            P("sp", "tp", None),
        ),
        out_specs=P(("sp", "tp"), None),
        check_vma=False,
    )
```

```python
import functools

import jax
import jax.numpy as jnp
from jax import lax
from jax.experimental import pallas as pl
from jax.experimental.pallas import tpu as pltpu
from jax.sharding import PartitionSpec as P

epsilon = 1e-06
MESH = pl.DeviceIdType.MESH
QUARTERS = 4


def shifted(value, axis, steps):
    count = lax.axis_size(axis)
    initial, last = (max(0, -steps), min(count, count - steps))
    return lax.ppermute(value, axis, [(source, source + steps) for source in range(initial, last)])


def moe_kernel(
    S,
    Z,
    C,
    packed,
    normed_ref,
    resid_ref,
    routes_ref,
    weights_ref,
    gate_hbm,
    up_hbm,
    down_hbm,
    out_ref,
    sendbuf,
    xbuf,
    wg,
    wu,
    wd,
    hid,
    mine,
    pout,
    pin,
    rbuf,
    fin,
    ret,
    w_sem,
    disp_send,
    disp_recv,
    agz_send,
    agz_recv,
    ags_send,
    ags_recv,
    rss_send,
    rss_recv,
    rsz_send,
    rsz_recv,
    ret_send,
    ret_recv,
):
    f32, bf16 = jnp.float32, jnp.bfloat16
    s_me = lax.axis_index("sp")
    t_me = lax.axis_index("tp")
    z_me, c_me = t_me // 2, t_me % 2
    half = Z // 2
    Q = S // QUARTERS
    W = normed_ref.shape[1]
    tokens = normed_ref.shape[0]
    F = down_hbm.shape[1]
    QR = Q * C
    M = Z * 2 * QR

    def sp_peer(steps):
        return (lax.rem(s_me + steps + S, S), t_me)

    def z_peer(steps):
        return (s_me, lax.rem(z_me + steps + Z, Z) * 2 + c_me)

    sibling = (s_me, z_me * 2 + 1 - c_me)

    loads = []
    if packed:
        tiles = F // 128
        for j in range(tiles):
            for k, src in enumerate((gate_hbm, up_hbm)):
                loads.append(
                    pltpu.make_async_copy(
                        src.at[0, :, pl.ds(j * 128, 128)],
                        wg.at[j, :, pl.ds(k * 128, 128)],
                        w_sem.at[2 * j + k],
                    )
                )
    else:
        tiles = 1
        loads.append(pltpu.make_async_copy(gate_hbm.at[0], wg.at[0], w_sem.at[0]))
        loads.append(pltpu.make_async_copy(up_hbm.at[0], wu.at[0], w_sem.at[1]))
    down_load = pltpu.make_async_copy(down_hbm.at[0], wd, w_sem.at[2 * tiles])
    for cp in loads:
        cp.start()
    down_load.start()

    barrier = pltpu.get_barrier_semaphore()
    peers = [sp_peer(j) for j in range(1, S)] + [z_peer(1), z_peer(-1), sibling]
    for peer in peers:
        pl.semaphore_signal(barrier, inc=1, device_id=peer, device_id_type=MESH)

    r0, r1 = routes_ref[0:1, :], routes_ref[1:2, :]
    w0, w1 = weights_ref[0:1, :], weights_ref[1:2, :]
    ids = s_me - lax.broadcasted_iota(jnp.int32, (S, tokens), 0)
    ids = jnp.where(ids < 0, ids + S, ids)
    hit0, hit1 = r0 == ids, r1 == ids
    named = jnp.where(hit0 | hit1, 1.0, 0.0)
    row_w = jnp.where(hit0, w0, 0.0) + jnp.where(hit1, w1, 0.0)
    earlier = jnp.where(
        lax.broadcasted_iota(jnp.int32, (tokens, tokens), 0)
        < lax.broadcasted_iota(jnp.int32, (tokens, tokens), 1),
        1.0,
        0.0,
    )
    rank = jnp.dot(named.astype(bf16), earlier.astype(bf16), preferred_element_type=f32)
    slot = lax.broadcasted_iota(jnp.int32, (C, tokens), 0).astype(f32)
    choose, weigh = [], []
    for j in range(S):
        pick = jnp.where(rank[j : j + 1, :] == slot, named[j : j + 1, :], 0.0)
        choose.append(pick)
        weigh.append(pick * row_w[j : j + 1, :])
    rows = normed_ref[...]
    sent = jnp.dot(
        jnp.concatenate(choose, axis=0).astype(bf16), rows, preferred_element_type=f32
    ).astype(bf16)
    xbuf[0, 0, 0, 0] = sent[0:C]
    for j in range(1, S):
        sendbuf[j] = sent[j * C : (j + 1) * C]

    pl.semaphore_wait(barrier, len(peers))

    sends = []

    def remote(src, dst, send_sem, recv_sem, peer):
        return pltpu.make_async_remote_copy(
            src_ref=src,
            dst_ref=dst,
            send_sem=send_sem,
            recv_sem=recv_sem,
            device_id=peer,
            device_id_type=MESH,
        )

    def start(cp):
        cp.start()
        sends.append(cp)

    def disp(j):
        return remote(
            sendbuf.at[j],
            xbuf.at[j // Q, 0, 0, j % Q],
            disp_send.at[j],
            disp_recv.at[j],
            sp_peer(-j),
        )

    def sign(d):
        return 1 if d == 0 else -1

    def reach(d, q):
        return half if d == q % 2 else half - 1

    def agz(d, k, q):
        return remote(
            xbuf.at[q, (-sign(d) * (k - 1)) % Z, 0],
            xbuf.at[q, (-sign(d) * k) % Z, 0],
            agz_send.at[d, k - 1, q],
            agz_recv.at[d, k - 1, q],
            z_peer(sign(d)),
        )

    def ags(q, r):
        return remote(
            xbuf.at[q, r, 0], xbuf.at[q, r, 1], ags_send.at[q, r], ags_recv.at[q, r], sibling
        )

    def rss(q, r):
        return remote(
            pout.at[q, r], pin.at[q, r], rss_send.at[q, r], rss_recv.at[q, r], sibling
        )

    def rsz(d, k, q):
        return remote(
            mine.at[q, (sign(d) * k) % Z],
            rbuf.at[d, k - 1, q],
            rsz_send.at[d, k - 1, q],
            rsz_recv.at[d, k - 1, q],
            z_peer(sign(d)),
        )

    def back(j):
        return remote(
            fin.at[j // Q, j % Q], ret.at[j], ret_send.at[j], ret_recv.at[j], sp_peer(j)
        )

    def first_hop(q):
        for i in range(Q):
            j = q * Q + i
            if j > 0:
                disp(j).wait_recv()
        for d in (q % 2, 1 - q % 2):
            if reach(d, q) >= 1:
                start(agz(d, 1, q))
        start(ags(q, 0))

    def forward(q, k):
        for d in (q % 2, 1 - q % 2):
            if reach(d, q) >= k:
                agz(d, k, q).wait_recv()
                if k < reach(d, q):
                    start(agz(d, k + 1, q))
                start(ags(q, (-sign(d) * k) % Z))

    def ready(q):
        for r in range(Z):
            ags(q, r).wait_recv()

    def ffn_up(q):
        if q == 0:
            for cp in loads:
                cp.wait()

        def tile(j, carry):
            x = xbuf[q].reshape(M, W)
            if packed:
                both = jnp.dot(x, wg[j], preferred_element_type=f32)
                g, u = both[:, :128], both[:, 128:]
                hid[:, pl.ds(pl.multiple_of(j * 128, 128), 128)] = (jax.nn.silu(g) * u).astype(bf16)
            else:
                g = jnp.dot(x, wg[0], preferred_element_type=f32)
                u = jnp.dot(x, wu[0], preferred_element_type=f32)
                hid[...] = (jax.nn.silu(g) * u).astype(bf16)
            return carry

        lax.fori_loop(0, tiles, tile, 0, unroll=True)

    step = 512

    def ffn_down(q):
        if q == 0:
            down_load.wait()

        def tile(n, carry):
            cols = pl.ds(pl.multiple_of(n * step, step), step)
            y = jnp.dot(hid[...], wd[:, cols], preferred_element_type=f32).astype(bf16)
            y = y.reshape(Z, 2, QR, step)
            mine[q, :, :, cols] = y[:, 0]
            pout[q, :, :, cols] = y[:, 1]
            return carry

        lax.fori_loop(0, W // step, tile, 0, unroll=True)
        for k in range(half, 0, -1):
            for r in sorted({k % Z, -k % Z}):
                start(rss(q, r))
        start(rss(q, 0))

    def pair_sum(q, r, extra=None):
        rss(q, r).wait_recv()
        total = mine[q, r].astype(f32) + pin[q, r].astype(f32)
        if extra is not None:
            total = total + extra[...].astype(f32)
        mine[q, r] = total.astype(bf16)

    def launch(q):
        for k in range(half, 0, -1):
            for d in (q % 2, 1 - q % 2):
                if reach(d, q) == k:
                    pair_sum(q, (sign(d) * k) % Z)
                    start(rsz(d, k, q))

    def relay(q):
        for k in range(half - 1, 0, -1):
            for d in (q % 2, 1 - q % 2):
                if reach(d, q) > k:
                    rsz(d, k + 1, q).wait_recv()
                    pair_sum(q, (sign(d) * k) % Z, rbuf.at[d, k, q])
                    start(rsz(d, k, q))

    def finish(q):
        rss(q, 0).wait_recv()
        total = mine[q, 0].astype(f32) + pin[q, 0].astype(f32)
        for d in (0, 1):
            if reach(d, q) >= 1:
                rsz(d, 1, q).wait_recv()
                total = total + rbuf[d, 0, q].astype(f32)
        done = total.astype(bf16).reshape(Q, C, W)
        if q == 0:
            ret[0] = done[0]
        fin[q] = done
        for i in range(Q):
            j = q * Q + i
            if j > 0:
                start(back(j))

    def far(f, q):
        for k in range(2, half + 1):
            f(q, k)

    for j in range(1, S):
        start(disp(j))
    first_hop(0)
    first_hop(1)
    forward(0, 1)
    first_hop(2)
    forward(1, 1)
    first_hop(3)
    far(forward, 0)
    ready(0)
    ffn_up(0)
    forward(2, 1)
    far(forward, 1)
    ffn_down(0)
    forward(3, 1)
    ready(1)
    launch(0)
    ffn_up(1)
    far(forward, 2)
    ffn_down(1)
    relay(0)
    far(forward, 3)
    ready(2)
    launch(1)
    ffn_up(2)
    ffn_down(2)
    relay(1)
    ready(3)
    launch(2)
    ffn_up(3)
    finish(0)
    ffn_down(3)
    relay(2)
    launch(3)
    finish(1)
    relay(3)
    finish(2)
    finish(3)

    spread = jnp.concatenate(weigh, axis=0).T
    high = spread.astype(bf16)
    low = (spread - high.astype(f32)).astype(bf16)
    for j in range(1, S):
        back(j).wait_recv()
    got = ret[...].reshape(S * C, W)
    mix = jnp.dot(high, got, preferred_element_type=f32) + jnp.dot(
        low, got, preferred_element_type=f32
    )
    out_ref[...] = (resid_ref[...].astype(f32) + mix).astype(bf16)
    for cp in sends:
        cp.wait_send()


def routed_experts(normed, residual, routes, route_weights, gate_w, up_w, down_w):
    S, T = lax.axis_size("sp"), lax.axis_size("tp")
    Z, half = T // 2, T // 4
    tokens, W = normed.shape
    C = routes.shape[1] * tokens // S
    Q = S // QUARTERS
    F = gate_w.shape[2]
    packed = F % 128 == 0
    tiles = F // 128 if packed else 1
    M = Z * 2 * Q * C
    bf16 = jnp.bfloat16
    vmem = pl.BlockSpec(memory_space=pltpu.VMEM)
    hbm = pl.BlockSpec(memory_space=pl.ANY)
    dma = pltpu.SemaphoreType.DMA
    quarter = (Q * C, W)
    return pl.pallas_call(
        functools.partial(moe_kernel, S, Z, C, packed),
        out_shape=jax.ShapeDtypeStruct((tokens, W), bf16),
        in_specs=[vmem] * 4 + [hbm] * 3,
        out_specs=vmem,
        scratch_shapes=[
            pltpu.VMEM((S, C, W), bf16),
            pltpu.VMEM((QUARTERS, Z, 2, Q, C, W), bf16),
            pltpu.VMEM((tiles, W, 256) if packed else (1, W, F), bf16),
            pltpu.VMEM((1, 16, 128) if packed else (1, W, F), bf16),
            pltpu.VMEM((F, W), bf16),
            pltpu.VMEM((M, F), bf16),
            pltpu.VMEM((QUARTERS, Z) + quarter, bf16),
            pltpu.VMEM((QUARTERS, Z) + quarter, bf16),
            pltpu.VMEM((QUARTERS, Z) + quarter, bf16),
            pltpu.VMEM((2, half, QUARTERS) + quarter, bf16),
            pltpu.VMEM((QUARTERS, Q, C, W), bf16),
            pltpu.VMEM((S, C, W), bf16),
            dma((2 * tiles + 1,)),
            dma((S,)),
            dma((S,)),
            dma((2, half, QUARTERS)),
            dma((2, half, QUARTERS)),
            dma((QUARTERS, Z)),
            dma((QUARTERS, Z)),
            dma((QUARTERS, Z)),
            dma((QUARTERS, Z)),
            dma((2, half, QUARTERS)),
            dma((2, half, QUARTERS)),
            dma((S,)),
            dma((S,)),
        ],
        compiler_params=pltpu.CompilerParams(
            collective_id=0, has_side_effects=True, vmem_limit_bytes=56 * 1024 * 1024
        ),
        name="routed_experts",
    )(normed, residual, routes.T, route_weights.T, gate_w, up_w, down_w)


def exchange_kernel(T, blocks_ref, out_ref, land, send_sem, recv_sem):
    s_me = lax.axis_index("sp")
    t_me = lax.axis_index("tp")
    barrier = pltpu.get_barrier_semaphore()
    for i in range(1, T):
        peer = (s_me, lax.rem(t_me + i, T))
        pl.semaphore_signal(barrier, inc=1, device_id=peer, device_id_type=MESH)
    pl.semaphore_wait(barrier, T - 1)
    copies = []
    for i in range(1, T):
        target = lax.rem(t_me + i, T)
        copies.append(
            pltpu.make_async_remote_copy(
                src_ref=blocks_ref.at[target],
                dst_ref=land.at[t_me],
                send_sem=send_sem.at[i],
                recv_sem=recv_sem.at[i],
                device_id=(s_me, target),
                device_id_type=MESH,
            )
        )
    for cp in copies:
        cp.start()
    land[t_me] = blocks_ref[t_me]
    for cp in copies:
        cp.wait()
    out_ref[...] = land[...]


def exchange(blocks):
    T = blocks.shape[0]
    vmem = pl.BlockSpec(memory_space=pltpu.VMEM)
    return pl.pallas_call(
        functools.partial(exchange_kernel, T),
        out_shape=jax.ShapeDtypeStruct(blocks.shape, blocks.dtype),
        in_specs=[vmem],
        out_specs=vmem,
        scratch_shapes=[
            pltpu.VMEM(blocks.shape, blocks.dtype),
            pltpu.SemaphoreType.DMA((T,)),
            pltpu.SemaphoreType.DMA((T,)),
        ],
        compiler_params=pltpu.CompilerParams(collective_id=1, has_side_effects=True),
        name="exchange",
    )(blocks)


class Link:
    def __init__(self):
        self.sent = []

    def copy(self, src, dst, send_sem, recv_sem, peer):
        return pltpu.make_async_remote_copy(
            src_ref=src,
            dst_ref=dst,
            send_sem=send_sem,
            recv_sem=recv_sem,
            device_id=peer,
            device_id_type=MESH,
        )

    def start(self, cp, cond=None):
        self.sent.append((cp, cond))
        if cond is None:
            cp.start()
        else:
            pl.when(cond)(cp.start)

    def drain(self):
        for cp, cond in self.sent:
            if cond is None:
                cp.wait_send()
            else:
                pl.when(cond)(cp.wait_send)


def fused_kernel(
    T,
    C,
    taps_n,
    value_ref,
    vgate_ref,
    taps_ref,
    gain_ref,
    bias_ref,
    routes_ref,
    weights_ref,
    egain_ref,
    stream_ref,
    outw_hbm,
    gate_hbm,
    up_hbm,
    down_hbm,
    out_ref,
    gbuf,
    halo_out,
    halo_in,
    cbuf,
    land,
    outw,
    res,
    meta,
    cho,
    hi,
    lo,
    tok,
    sbuf,
    X,
    wg,
    wd,
    hid,
    mine,
    pout,
    pin,
    ret,
    tot,
    tout,
    tin,
    tmid,
    rin,
    w_sem,
    halo_sem,
    ex_send,
    ex_recv,
    meta_send,
    meta_recv,
    tz_send,
    tz_recv,
    pl_send,
    pl_recv,
    sx_send,
    sx_recv,
    sy_send,
    sy_recv,
    rt_send,
    rt_recv,
    zo_send,
    zo_recv,
    tm_recv,
    cx_send,
    cx_recv,
    nr_send,
    nr_recv,
):
    f32, bf16 = jnp.float32, jnp.bfloat16
    s = lax.axis_index("sp")
    t = lax.axis_index("tp")
    z, c = t // 2, t % 2
    Z, J = T // 2, 4
    gy, gx = s // 2, s % 2
    W = out_ref.shape[1]
    tokens = out_ref.shape[0]
    F = wd.shape[0]
    tiles = F // 128
    ch, run = value_ref.shape
    rim = gbuf.shape[0] - run
    link = Link()

    def plane(j):
        return (lax.rem(gy + j // 2, 2) * 2 + lax.rem(gx + j % 2, 2), t)

    def at_z(zt):
        return (s, zt * 2 + c)

    sibling = (s, z * 2 + 1 - c)

    zp = [z, 1 + z % 2, 2 + z % 2 - 2 * (z // 2), 3 - 3 * (z % 2)]
    middle = (z >= 1) & (z <= Z - 2)

    outw_load = pltpu.make_async_copy(outw_hbm, outw, w_sem.at[2 * tiles + 1])
    outw_load.start()
    loads = []
    for j in range(tiles):
        for k, src in enumerate((gate_hbm, up_hbm)):
            loads.append(
                pltpu.make_async_copy(
                    src.at[0, :, pl.ds(j * 128, 128)],
                    wg.at[j, :, pl.ds(k * 128, 128)],
                    w_sem.at[2 * j + k],
                )
            )
    down_load = pltpu.make_async_copy(down_hbm.at[0], wd, w_sem.at[2 * tiles])
    for cp in loads:
        cp.start()
    down_load.start()

    barrier = pltpu.get_barrier_semaphore()
    peers = [plane(j) for j in range(1, J)] + [(s, lax.rem(t + i, T)) for i in range(1, T)]
    for peer in peers:
        pl.semaphore_signal(barrier, inc=1, device_id=peer, device_id_type=MESH)

    gated = (
        value_ref[...].astype(f32) * jax.nn.sigmoid(vgate_ref[...].astype(f32))
    ).astype(bf16)
    turned = gated.astype(f32).T
    gbuf[rim:, :] = turned
    halo_out[...] = turned[run - rim :, :].astype(bf16)
    meta[z, 0:2, 0:tokens] = routes_ref[...].astype(f32)
    meta[z, 2:4, 0:tokens] = weights_ref[...]

    pl.semaphore_wait(barrier, len(peers))

    S = J
    halo = link.copy(
        halo_out, halo_in, halo_sem.at[0], halo_sem.at[1], (lax.rem(s + 1, S), t)
    )
    link.start(halo, s < S - 1)

    def mz(i, zs):
        return link.copy(
            meta.at[z], meta.at[z], meta_send.at[i - 1], meta_recv.at[z], at_z(zs)
        )

    for i in range(1, Z):
        link.start(mz(i, lax.rem(z + i, Z)))

    def conv(b):
        acc = jnp.zeros((tokens, ch), f32)
        for j in range(taps_n):
            lead = rim - (taps_n - 1) + b * tokens + j
            acc = acc + taps_ref[j : j + 1, :] * gbuf[lead : lead + tokens, :]
        cbuf[b] = acc.astype(bf16)

    for b in range(1, T):
        conv(b)

    @pl.when(s > 0)
    def _():
        halo.wait_recv()
        gbuf[0:rim, :] = halo_in[...].astype(f32)

    @pl.when(s == 0)
    def _():
        gbuf[0:rim, :] = jnp.zeros((rim, ch), f32)

    conv(0)

    exchanges = []
    for i in range(1, T):
        target = lax.rem(t + i, T)
        cp = link.copy(
            cbuf.at[target], land.at[t], ex_send.at[i - 1], ex_recv.at[i - 1], (s, target)
        )
        link.start(cp)
        exchanges.append(cp)
    land[t] = cbuf[t]

    metas = [
        link.copy(
            meta.at[zp[p]], meta.at[zp[p]], meta_send.at[p - 1], meta_recv.at[zp[p]], at_z(zp[p])
        )
        for p in range(1, Z)
    ]

    row = lax.broadcasted_iota(jnp.int32, (J, tokens), 0)
    ids = (((gy + (row >> 1)) & 1) * 2 + ((gx + (row & 1)) & 1)).astype(f32)
    earlier = jnp.where(
        lax.broadcasted_iota(jnp.int32, (tokens, tokens), 0)
        < lax.broadcasted_iota(jnp.int32, (tokens, tokens), 1),
        1.0,
        0.0,
    ).astype(bf16)
    slot = lax.broadcasted_iota(jnp.int32, (C, tokens), 0).astype(f32)
    def matrices(p):
        if p > 0:
            metas[p - 1].wait_recv()
        m = meta[zp[p]]
        r0, r1 = m[0:1, :tokens], m[1:2, :tokens]
        w0, w1 = m[2:3, :tokens], m[3:4, :tokens]
        hit0, hit1 = r0 == ids, r1 == ids
        named = jnp.where(hit0 | hit1, 1.0, 0.0)
        row_w = jnp.where(hit0, w0, 0.0) + jnp.where(hit1, w1, 0.0)
        rank = jnp.dot(named.astype(bf16), earlier, preferred_element_type=f32)
        choose, weigh = [], []
        for j in range(J):
            pick = jnp.where(rank[j : j + 1, :] == slot, named[j : j + 1, :], 0.0)
            choose.append(pick)
            weigh.append(pick * row_w[j : j + 1, :])
        cho[p] = jnp.concatenate(choose, axis=0).astype(bf16)
        spread = jnp.concatenate(weigh, axis=0).T
        high = spread.astype(bf16)
        hi[p] = high
        lo[p] = (spread - high.astype(f32)).astype(bf16)

    matrices(0)

    for cp in exchanges:
        cp.wait_recv()
    whole = jnp.concatenate([land[i] for i in range(T)], axis=1).astype(f32)
    center = jnp.mean(whole, axis=1, keepdims=True)
    whole = whole - center
    var = jnp.mean(whole * whole, axis=1, keepdims=True)
    act = jax.nn.silu(
        whole * lax.rsqrt(var + epsilon) * gain_ref[...] + bias_ref[...]
    ).astype(bf16)
    outw_load.wait()
    step = 512
    square = jnp.zeros((tokens, 1), f32)
    for n in range(W // step):
        cut = slice(n * step, (n + 1) * step)
        r = (
            stream_ref[:, cut].astype(f32)
            + jnp.dot(act, outw[:, cut], preferred_element_type=f32)
        ).astype(bf16)
        res[:, cut] = r
        rf = r.astype(f32)
        square = square + jnp.sum(rf * rf, axis=1, keepdims=True)
    scale = lax.rsqrt(square * (1.0 / W) + epsilon)
    for n in range(W // step):
        cut = slice(n * step, (n + 1) * step)
        tok[z, :, cut] = (res[:, cut].astype(f32) * scale * egain_ref[:, cut]).astype(bf16)

    H = pout.shape[0]
    span = W // H

    def half(h):
        return pl.ds(h * span, span)

    def sign(d):
        return 1 if d == 0 else -1

    def inside(v):
        return (v >= 0) & (v < Z)

    def tz(d, k, h, steps):
        block = lax.rem(z - sign(d) * steps + Z, Z)
        return link.copy(
            tok.at[block, :, half(h)],
            tok.at[block, :, half(h)],
            tz_send.at[d, k - 1, h],
            tz_recv.at[d, k - 1, h],
            at_z(lax.rem(z + sign(d) + Z, Z)),
        )

    def arrive(k, h):
        for d in (0, 1):
            sg = sign(d)
            pl.when(inside(z - sg * k))(tz(d, k, h, k).wait_recv)
            if k < Z - 1:
                link.start(tz(d, k + 1, h, k), inside(z - sg * k) & inside(z + sg))

    def pland(p, j, h):
        return link.copy(
            sbuf.at[p, j - 1, :, half(h)],
            X.at[p, j, 0, :, half(h)],
            pl_send.at[p, j - 1, h],
            pl_recv.at[p, j - 1, h],
            plane(j),
        )

    def sibx(p, j, h):
        return link.copy(
            X.at[p, j, 0, :, half(h)],
            X.at[p, j, 1, :, half(h)],
            sx_send.at[p, j, h],
            sx_recv.at[p, j, h],
            sibling,
        )

    def select(p, h):
        for n in range(span // step):
            cut = slice(h * span + n * step, h * span + (n + 1) * step)
            sel = jnp.dot(cho[p], tok[zp[p], :, cut], preferred_element_type=f32).astype(bf16)
            X[p, 0, 0, :, cut] = sel[0:C]
            for j in range(1, J):
                sbuf[p, j - 1, :, cut] = sel[j * C : (j + 1) * C]
        for j in (1, 2) if p == 1 else (3, 1, 2):
            link.start(pland(p, j, h))
        link.start(sibx(p, 0, h))

    def corner(d, h):
        return link.copy(
            X.at[0, 3, 0, :, half(h)],
            X.at[1, 3, 0, :, half(h)],
            cx_send.at[d, h],
            cx_recv.at[h],
            at_z(lax.rem(z + sign(d) + Z, Z)),
        )

    def forward(p, h):
        for j in (3, 1, 2):
            if p == 1 and j == 3:
                corner(0, h).wait_recv()
            else:
                pland(p, j, h).wait_recv()
            link.start(sibx(p, j, h))
            if p == 0 and j == 3:
                for d in (0, 1):
                    link.start(corner(d, h), middle)

    def gather(p):
        for h in range(H):
            for j in range(J):
                sibx(p, j, h).wait_recv()

    M = J * 2 * C

    def ffn_up(p, start=0, stop=tiles):
        if p == 0 and start == 0:
            for cp in loads:
                cp.wait()
        for j in range(start, stop):
            x = X[p].reshape(M, W)
            both = jnp.dot(x, wg[j], preferred_element_type=f32)
            g, u = both[:, :128], both[:, 128:]
            hid[:, j * 128 : (j + 1) * 128] = (jax.nn.silu(g) * u).astype(bf16)

    def siby(p, h):
        return link.copy(
            pout.at[h, p], pin.at[h, p], sy_send.at[p, h], sy_recv.at[p, h], sibling
        )

    def ffn_down(p, h):
        if p == 0 and h == 0:
            down_load.wait()
        for n in range(span // step):
            cut = slice(n * step, (n + 1) * step)
            full = slice(h * span + n * step, h * span + (n + 1) * step)
            y = jnp.dot(hid[...], wd[:, full], preferred_element_type=f32).astype(bf16)
            y = y.reshape(J, 2, C, step)
            mine[h, p, :, :, cut] = y[:, 0]
            pout[h, p, :, :, cut] = y[:, 1]
        link.start(siby(p, h))

    def back(p, j, h):
        return link.copy(
            mine.at[h, p, j],
            ret.at[h, p, j],
            rt_send.at[p, j - 1, h],
            rt_recv.at[p, j - 1, h],
            plane(j),
        )

    def neighbour_rows(spot, h):
        return link.copy(
            mine.at[h, 1], rin.at[spot, h], nr_send.at[h], nr_recv.at[spot, h], at_z(zp[1])
        )

    def give(p, h):
        siby(p, h).wait_recv()
        total = mine[h, p].astype(f32) + pin[h, p].astype(f32)
        if p == 1:
            mine[h, 1] = total.astype(bf16)
            link.start(neighbour_rows(z // 2, h))
            return
        if p == 0:

            @pl.when(middle)
            def _():
                neighbour_rows(0, h).wait_recv()
                neighbour_rows(1, h).wait_recv()
                mine[h, 0] = (total + rin[0, h].astype(f32) + rin[1, h].astype(f32)).astype(bf16)

            @pl.when(jnp.logical_not(middle))
            def _():
                mine[h, 0] = total.astype(bf16)

        else:
            mine[h, p] = total.astype(bf16)
        ret[h, p, 0] = mine[h, p, 0]
        for j in (3, 1, 2):
            link.start(back(p, j, h))

    def zout(p, h):
        return link.copy(
            tout.at[h, p - 2], tin.at[h, z], zo_send.at[p - 2, h], zo_recv.at[z, h], at_z(zp[p])
        )

    def zin(p, h):
        return link.copy(
            tout.at[h, 0], tin.at[h, zp[p]], zo_send.at[0, h], zo_recv.at[zp[p], h], at_z(zp[p])
        )

    def zmid(h):
        return link.copy(
            tout.at[h, 1], tmid.at[h], zo_send.at[1, h], tm_recv.at[h], at_z(zp[1])
        )

    def mixed_part(p, h):
        for j in (3, 1, 2):
            back(p, j, h).wait_recv()
        got = ret[h, p].reshape(J * C, span)
        return jnp.dot(hi[p], got, preferred_element_type=f32) + jnp.dot(
            lo[p], got, preferred_element_type=f32
        )

    end = jnp.logical_not(middle)

    def combine(p, h):
        tout[h, p - 2] = mixed_part(p, h).astype(bf16)
        if p == 2:
            link.start(zout(2, h), end)
        else:
            link.start(zmid(h), end)
            link.start(zout(3, h), middle)

    def merge(h):
        @pl.when(middle)
        def _():
            zmid(h).wait_recv()
            tout[h, 0] = (tout[h, 0].astype(f32) + tmid[h].astype(f32)).astype(bf16)

        link.start(zout(2, h), middle)

    for h in range(H):
        for d in (0, 1):
            link.start(tz(d, 1, h, 0), inside(z + sign(d)))
    select(0, 0)
    select(0, 1)
    matrices(1)
    matrices(2)
    matrices(3)
    arrive(1, 0)
    select(1, 0)
    forward(0, 0)
    arrive(1, 1)
    select(1, 1)
    forward(0, 1)
    gather(0)
    ffn_up(0)
    arrive(2, 0)
    select(2, 0)
    forward(1, 0)
    ffn_down(0, 0)
    arrive(2, 1)
    select(2, 1)
    ffn_down(0, 1)
    forward(1, 1)
    gather(1)
    arrive(3, 0)
    select(3, 0)
    ffn_up(1)
    arrive(3, 1)
    select(3, 1)
    forward(2, 0)
    ffn_down(1, 0)
    forward(2, 1)
    ffn_down(1, 1)
    gather(2)
    give(1, 0)
    give(1, 1)
    ffn_up(2)
    forward(3, 0)
    ffn_down(2, 0)
    forward(3, 1)
    ffn_down(2, 1)
    give(2, 0)
    gather(3)
    ffn_up(3, 0, tiles // 2)
    give(2, 1)
    ffn_up(3, tiles // 2, tiles)
    ffn_down(3, 0)
    ffn_down(3, 1)
    give(3, 0)
    combine(2, 0)
    combine(2, 1)
    give(3, 1)
    combine(3, 0)
    give(0, 0)
    combine(3, 1)
    give(0, 1)
    for h in range(H):
        merge(h)
        cut = slice(h * span, (h + 1) * span)
        tot[:, cut] = res[:, cut].astype(f32) + mixed_part(0, h)
    for h in range(H):
        cut = slice(h * span, (h + 1) * span)
        zin(2, h).wait_recv()
        acc = tot[:, cut] + tin[h, zp[2]].astype(f32)

        @pl.when(middle)
        def _():
            out_ref[:, cut] = acc.astype(bf16)

        @pl.when(end)
        def _():
            zin(1, h).wait_recv()
            out_ref[:, cut] = (acc + tin[h, zp[1]].astype(f32)).astype(bf16)

    link.drain()


def fused(
    conv_value, conv_gate, conv_taps, norm_gain, norm_bias, out_weight, stream,
    routes, route_weights, expert_gain, gate_w, up_w, down_w,
):
    T = lax.axis_size("tp")
    S, Z = lax.axis_size("sp"), T // 2
    tokens, W = stream.shape
    C = routes.shape[1] * tokens // S
    F = gate_w.shape[2]
    ch, run = conv_value.shape
    taps_n = conv_taps.shape[1]
    rim = -(-(taps_n - 1) // 16) * 16
    tiles = F // 128
    H = 2
    span = W // H
    f32, bf16 = jnp.float32, jnp.bfloat16
    vmem = pl.BlockSpec(memory_space=pltpu.VMEM)
    hbm = pl.BlockSpec(memory_space=pl.ANY)
    dma = pltpu.SemaphoreType.DMA
    rows = (H, Z, S, C, span)
    return pl.pallas_call(
        functools.partial(fused_kernel, T, C, taps_n),
        out_shape=jax.ShapeDtypeStruct((tokens, W), bf16),
        in_specs=[vmem] * 9 + [hbm] * 4,
        out_specs=vmem,
        scratch_shapes=[
            pltpu.VMEM((rim + run, ch), f32),
            pltpu.VMEM((rim, ch), bf16),
            pltpu.VMEM((rim, ch), bf16),
            pltpu.VMEM((T, tokens, ch), bf16),
            pltpu.VMEM((T, tokens, ch), bf16),
            pltpu.VMEM(out_weight.shape, bf16),
            pltpu.VMEM((tokens, W), bf16),
            pltpu.VMEM((Z, 8, 128), f32),
            pltpu.VMEM((Z, S * C, tokens), bf16),
            pltpu.VMEM((Z, tokens, S * C), bf16),
            pltpu.VMEM((Z, tokens, S * C), bf16),
            pltpu.VMEM((Z, tokens, W), bf16),
            pltpu.VMEM((Z, S - 1, C, W), bf16),
            pltpu.VMEM((Z, S, 2, C, W), bf16),
            pltpu.VMEM((tiles, W, 256), bf16),
            pltpu.VMEM((F, W), bf16),
            pltpu.VMEM((S * 2 * C, F), bf16),
            pltpu.VMEM(rows, bf16),
            pltpu.VMEM(rows, bf16),
            pltpu.VMEM(rows, bf16),
            pltpu.VMEM(rows, bf16),
            pltpu.VMEM((tokens, W), f32),
            pltpu.VMEM((H, 2, tokens, span), bf16),
            pltpu.VMEM((H, Z, tokens, span), bf16),
            pltpu.VMEM((H, tokens, span), bf16),
            pltpu.VMEM((2, H, S, C, span), bf16),
            dma((2 * tiles + 2,)),
            dma((2,)),
            dma((T - 1,)),
            dma((T - 1,)),
            dma((Z - 1,)),
            dma((Z,)),
            dma((2, Z - 1, H)),
            dma((2, Z - 1, H)),
            dma((Z, S - 1, H)),
            dma((Z, S - 1, H)),
            dma((Z, S, H)),
            dma((Z, S, H)),
            dma((Z, H)),
            dma((Z, H)),
            dma((Z, S - 1, H)),
            dma((Z, S - 1, H)),
            dma((2, H)),
            dma((Z, H)),
            dma((H,)),
            dma((2, H)),
            dma((H,)),
            dma((H,)),
            dma((2, H)),
        ],
        compiler_params=pltpu.CompilerParams(
            collective_id=2, has_side_effects=True, vmem_limit_bytes=60 * 1024 * 1024
        ),
        name="fused_block",
    )(
        conv_value, conv_gate, conv_taps.T, norm_gain.reshape(1, -1), norm_bias.reshape(1, -1),
        routes.T, route_weights.T, expert_gain.reshape(1, -1), stream,
        out_weight, gate_w, up_w, down_w,
    )


def per_device(
    conv_value,
    conv_gate,
    conv_taps,
    norm_gain,
    norm_bias,
    out_weight,
    stream,
    routes,
    route_weights,
    expert_gain,
    expert_gate,
    expert_up,
    expert_down,
):
    square_plane = lax.axis_size("sp") == 4 and lax.axis_size("tp") == 8
    if square_plane and expert_gate.shape[2] % 128 == 0 and conv_value.shape[0] % 128 == 0:
        return fused(
            conv_value, conv_gate, conv_taps, norm_gain, norm_bias, out_weight, stream,
            routes, route_weights, expert_gain, expert_gate, expert_up, expert_down,
        )
    f32 = jnp.float32
    local_ch = conv_value.shape[0]
    run_len = conv_value.shape[1]
    kernel_len = conv_taps.shape[1]
    gated_input = (conv_value.astype(f32) * jax.nn.sigmoid(conv_gate.astype(f32))).astype(
        jnp.bfloat16
    )
    left_rim = shifted(gated_input[:, run_len - (kernel_len - 1) :], "sp", 1)
    padded = jnp.concatenate([left_rim, gated_input], axis=1).astype(f32)
    conv_sum = jnp.zeros((local_ch, run_len), f32)
    for offset in range(kernel_len):
        conv_sum = (
            conv_sum + conv_taps[:, offset : offset + 1] * padded[:, offset : offset + run_len]
        )
    conv_out = conv_sum.astype(jnp.bfloat16)
    parts = lax.axis_size("tp")
    tok_rows = run_len // parts
    pieces = exchange(conv_out.T.reshape(parts, tok_rows, local_ch))
    whole_conv = pieces.transpose(1, 0, 2).reshape(tok_rows, parts * local_ch).astype(f32)
    center = jnp.mean(whole_conv, axis=1, keepdims=True)
    spread = jnp.mean((whole_conv - center) ** 2, axis=1, keepdims=True)
    scaled = (whole_conv - center) * lax.rsqrt(spread + epsilon) * norm_gain + norm_bias
    token_major = jax.nn.silu(scaled).astype(jnp.bfloat16)
    projected = jnp.dot(token_major, out_weight, preferred_element_type=f32)
    residual = (stream.astype(f32) + projected).astype(jnp.bfloat16)
    res_float = residual.astype(f32)
    normed = (
        res_float
        * lax.rsqrt(jnp.mean(res_float * res_float, axis=1, keepdims=True) + epsilon)
        * expert_gain
    ).astype(jnp.bfloat16)
    return routed_experts(
        normed, residual, routes, route_weights, expert_gate, expert_up, expert_down
    )


def solution(mesh):
    return jax.shard_map(
        per_device,
        mesh=mesh,
        in_specs=(
            P("tp", "sp"),
            P("tp", "sp"),
            P("tp", None),
            P(),
            P(),
            P(),
            P(("sp", "tp"), None),
            P(("sp", "tp"), None),
            P(("sp", "tp"), None),
            P(),
            P("sp", None, "tp"),
            P("sp", None, "tp"),
            P("sp", "tp", None),
        ),
        out_specs=P(("sp", "tp"), None),
        check_vma=False,
    )
```

```python
import functools

import jax
import jax.numpy as jnp
from jax import lax
from jax.experimental import pallas as pl
from jax.experimental.pallas import tpu as pltpu
from jax.sharding import PartitionSpec as P

epsilon = 1e-06
MESH = pl.DeviceIdType.MESH
QUARTERS = 4


def shifted(value, axis, steps):
    count = lax.axis_size(axis)
    initial, last = (max(0, -steps), min(count, count - steps))
    return lax.ppermute(value, axis, [(source, source + steps) for source in range(initial, last)])


def moe_kernel(
    S,
    Z,
    C,
    packed,
    normed_ref,
    resid_ref,
    routes_ref,
    weights_ref,
    gate_hbm,
    up_hbm,
    down_hbm,
    out_ref,
    sendbuf,
    xbuf,
    wg,
    wu,
    wd,
    hid,
    mine,
    pout,
    pin,
    rbuf,
    fin,
    ret,
    w_sem,
    disp_send,
    disp_recv,
    agz_send,
    agz_recv,
    ags_send,
    ags_recv,
    rss_send,
    rss_recv,
    rsz_send,
    rsz_recv,
    ret_send,
    ret_recv,
):
    f32, bf16 = jnp.float32, jnp.bfloat16
    s_me = lax.axis_index("sp")
    t_me = lax.axis_index("tp")
    z_me, c_me = t_me // 2, t_me % 2
    half = Z // 2
    Q = S // QUARTERS
    W = normed_ref.shape[1]
    tokens = normed_ref.shape[0]
    F = down_hbm.shape[1]
    QR = Q * C
    M = Z * 2 * QR

    def sp_peer(steps):
        return (lax.rem(s_me + steps + S, S), t_me)

    def z_peer(steps):
        return (s_me, lax.rem(z_me + steps + Z, Z) * 2 + c_me)

    sibling = (s_me, z_me * 2 + 1 - c_me)

    loads = []
    if packed:
        tiles = F // 128
        for j in range(tiles):
            for k, src in enumerate((gate_hbm, up_hbm)):
                loads.append(
                    pltpu.make_async_copy(
                        src.at[0, :, pl.ds(j * 128, 128)],
                        wg.at[j, :, pl.ds(k * 128, 128)],
                        w_sem.at[2 * j + k],
                    )
                )
    else:
        tiles = 1
        loads.append(pltpu.make_async_copy(gate_hbm.at[0], wg.at[0], w_sem.at[0]))
        loads.append(pltpu.make_async_copy(up_hbm.at[0], wu.at[0], w_sem.at[1]))
    down_load = pltpu.make_async_copy(down_hbm.at[0], wd, w_sem.at[2 * tiles])
    for cp in loads:
        cp.start()
    down_load.start()

    barrier = pltpu.get_barrier_semaphore()
    peers = [sp_peer(j) for j in range(1, S)] + [z_peer(1), z_peer(-1), sibling]
    for peer in peers:
        pl.semaphore_signal(barrier, inc=1, device_id=peer, device_id_type=MESH)

    r0, r1 = routes_ref[0:1, :], routes_ref[1:2, :]
    w0, w1 = weights_ref[0:1, :], weights_ref[1:2, :]
    ids = s_me - lax.broadcasted_iota(jnp.int32, (S, tokens), 0)
    ids = jnp.where(ids < 0, ids + S, ids)
    hit0, hit1 = r0 == ids, r1 == ids
    named = jnp.where(hit0 | hit1, 1.0, 0.0)
    row_w = jnp.where(hit0, w0, 0.0) + jnp.where(hit1, w1, 0.0)
    earlier = jnp.where(
        lax.broadcasted_iota(jnp.int32, (tokens, tokens), 0)
        < lax.broadcasted_iota(jnp.int32, (tokens, tokens), 1),
        1.0,
        0.0,
    )
    rank = jnp.dot(named.astype(bf16), earlier.astype(bf16), preferred_element_type=f32)
    slot = lax.broadcasted_iota(jnp.int32, (C, tokens), 0).astype(f32)
    choose, weigh = [], []
    for j in range(S):
        pick = jnp.where(rank[j : j + 1, :] == slot, named[j : j + 1, :], 0.0)
        choose.append(pick)
        weigh.append(pick * row_w[j : j + 1, :])
    rows = normed_ref[...]
    sent = jnp.dot(
        jnp.concatenate(choose, axis=0).astype(bf16), rows, preferred_element_type=f32
    ).astype(bf16)
    xbuf[0, 0, 0, 0] = sent[0:C]
    for j in range(1, S):
        sendbuf[j] = sent[j * C : (j + 1) * C]

    pl.semaphore_wait(barrier, len(peers))

    sends = []

    def remote(src, dst, send_sem, recv_sem, peer):
        return pltpu.make_async_remote_copy(
            src_ref=src,
            dst_ref=dst,
            send_sem=send_sem,
            recv_sem=recv_sem,
            device_id=peer,
            device_id_type=MESH,
        )

    def start(cp):
        cp.start()
        sends.append(cp)

    def disp(j):
        return remote(
            sendbuf.at[j],
            xbuf.at[j // Q, 0, 0, j % Q],
            disp_send.at[j],
            disp_recv.at[j],
            sp_peer(-j),
        )

    def sign(d):
        return 1 if d == 0 else -1

    def reach(d, q):
        return half if d == q % 2 else half - 1

    def agz(d, k, q):
        return remote(
            xbuf.at[q, (-sign(d) * (k - 1)) % Z, 0],
            xbuf.at[q, (-sign(d) * k) % Z, 0],
            agz_send.at[d, k - 1, q],
            agz_recv.at[d, k - 1, q],
            z_peer(sign(d)),
        )

    def ags(q, r):
        return remote(
            xbuf.at[q, r, 0], xbuf.at[q, r, 1], ags_send.at[q, r], ags_recv.at[q, r], sibling
        )

    def rss(q, r):
        return remote(
            pout.at[q, r], pin.at[q, r], rss_send.at[q, r], rss_recv.at[q, r], sibling
        )

    def rsz(d, k, q):
        return remote(
            mine.at[q, (sign(d) * k) % Z],
            rbuf.at[d, k - 1, q],
            rsz_send.at[d, k - 1, q],
            rsz_recv.at[d, k - 1, q],
            z_peer(sign(d)),
        )

    def back(j):
        return remote(
            fin.at[j // Q, j % Q], ret.at[j], ret_send.at[j], ret_recv.at[j], sp_peer(j)
        )

    def first_hop(q):
        for i in range(Q):
            j = q * Q + i
            if j > 0:
                disp(j).wait_recv()
        for d in (q % 2, 1 - q % 2):
            if reach(d, q) >= 1:
                start(agz(d, 1, q))
        start(ags(q, 0))

    def forward(q, k):
        for d in (q % 2, 1 - q % 2):
            if reach(d, q) >= k:
                agz(d, k, q).wait_recv()
                if k < reach(d, q):
                    start(agz(d, k + 1, q))
                start(ags(q, (-sign(d) * k) % Z))

    def ready(q):
        for r in range(Z):
            ags(q, r).wait_recv()

    def ffn_up(q):
        if q == 0:
            for cp in loads:
                cp.wait()

        def tile(j, carry):
            x = xbuf[q].reshape(M, W)
            if packed:
                both = jnp.dot(x, wg[j], preferred_element_type=f32)
                g, u = both[:, :128], both[:, 128:]
                hid[:, pl.ds(pl.multiple_of(j * 128, 128), 128)] = (jax.nn.silu(g) * u).astype(bf16)
            else:
                g = jnp.dot(x, wg[0], preferred_element_type=f32)
                u = jnp.dot(x, wu[0], preferred_element_type=f32)
                hid[...] = (jax.nn.silu(g) * u).astype(bf16)
            return carry

        lax.fori_loop(0, tiles, tile, 0, unroll=True)

    step = 512

    def ffn_down(q):
        if q == 0:
            down_load.wait()

        def tile(n, carry):
            cols = pl.ds(pl.multiple_of(n * step, step), step)
            y = jnp.dot(hid[...], wd[:, cols], preferred_element_type=f32).astype(bf16)
            y = y.reshape(Z, 2, QR, step)
            mine[q, :, :, cols] = y[:, 0]
            pout[q, :, :, cols] = y[:, 1]
            return carry

        lax.fori_loop(0, W // step, tile, 0, unroll=True)
        for k in range(half, 0, -1):
            for r in sorted({k % Z, -k % Z}):
                start(rss(q, r))
        start(rss(q, 0))

    def pair_sum(q, r, extra=None):
        rss(q, r).wait_recv()
        total = mine[q, r].astype(f32) + pin[q, r].astype(f32)
        if extra is not None:
            total = total + extra[...].astype(f32)
        mine[q, r] = total.astype(bf16)

    def launch(q):
        for k in range(half, 0, -1):
            for d in (q % 2, 1 - q % 2):
                if reach(d, q) == k:
                    pair_sum(q, (sign(d) * k) % Z)
                    start(rsz(d, k, q))

    def relay(q):
        for k in range(half - 1, 0, -1):
            for d in (q % 2, 1 - q % 2):
                if reach(d, q) > k:
                    rsz(d, k + 1, q).wait_recv()
                    pair_sum(q, (sign(d) * k) % Z, rbuf.at[d, k, q])
                    start(rsz(d, k, q))

    def finish(q):
        rss(q, 0).wait_recv()
        total = mine[q, 0].astype(f32) + pin[q, 0].astype(f32)
        for d in (0, 1):
            if reach(d, q) >= 1:
                rsz(d, 1, q).wait_recv()
                total = total + rbuf[d, 0, q].astype(f32)
        done = total.astype(bf16).reshape(Q, C, W)
        if q == 0:
            ret[0] = done[0]
        fin[q] = done
        for i in range(Q):
            j = q * Q + i
            if j > 0:
                start(back(j))

    def far(f, q):
        for k in range(2, half + 1):
            f(q, k)

    for j in range(1, S):
        start(disp(j))
    first_hop(0)
    first_hop(1)
    forward(0, 1)
    first_hop(2)
    forward(1, 1)
    first_hop(3)
    far(forward, 0)
    ready(0)
    ffn_up(0)
    forward(2, 1)
    far(forward, 1)
    ffn_down(0)
    forward(3, 1)
    ready(1)
    launch(0)
    ffn_up(1)
    far(forward, 2)
    ffn_down(1)
    relay(0)
    far(forward, 3)
    ready(2)
    launch(1)
    ffn_up(2)
    ffn_down(2)
    relay(1)
    ready(3)
    launch(2)
    ffn_up(3)
    finish(0)
    ffn_down(3)
    relay(2)
    launch(3)
    finish(1)
    relay(3)
    finish(2)
    finish(3)

    spread = jnp.concatenate(weigh, axis=0).T
    high = spread.astype(bf16)
    low = (spread - high.astype(f32)).astype(bf16)
    for j in range(1, S):
        back(j).wait_recv()
    got = ret[...].reshape(S * C, W)
    mix = jnp.dot(high, got, preferred_element_type=f32) + jnp.dot(
        low, got, preferred_element_type=f32
    )
    out_ref[...] = (resid_ref[...].astype(f32) + mix).astype(bf16)
    for cp in sends:
        cp.wait_send()


def routed_experts(normed, residual, routes, route_weights, gate_w, up_w, down_w):
    S, T = lax.axis_size("sp"), lax.axis_size("tp")
    Z, half = T // 2, T // 4
    tokens, W = normed.shape
    C = routes.shape[1] * tokens // S
    Q = S // QUARTERS
    F = gate_w.shape[2]
    packed = F % 128 == 0
    tiles = F // 128 if packed else 1
    M = Z * 2 * Q * C
    bf16 = jnp.bfloat16
    vmem = pl.BlockSpec(memory_space=pltpu.VMEM)
    hbm = pl.BlockSpec(memory_space=pl.ANY)
    dma = pltpu.SemaphoreType.DMA
    quarter = (Q * C, W)
    return pl.pallas_call(
        functools.partial(moe_kernel, S, Z, C, packed),
        out_shape=jax.ShapeDtypeStruct((tokens, W), bf16),
        in_specs=[vmem] * 4 + [hbm] * 3,
        out_specs=vmem,
        scratch_shapes=[
            pltpu.VMEM((S, C, W), bf16),
            pltpu.VMEM((QUARTERS, Z, 2, Q, C, W), bf16),
            pltpu.VMEM((tiles, W, 256) if packed else (1, W, F), bf16),
            pltpu.VMEM((1, 16, 128) if packed else (1, W, F), bf16),
            pltpu.VMEM((F, W), bf16),
            pltpu.VMEM((M, F), bf16),
            pltpu.VMEM((QUARTERS, Z) + quarter, bf16),
            pltpu.VMEM((QUARTERS, Z) + quarter, bf16),
            pltpu.VMEM((QUARTERS, Z) + quarter, bf16),
            pltpu.VMEM((2, half, QUARTERS) + quarter, bf16),
            pltpu.VMEM((QUARTERS, Q, C, W), bf16),
            pltpu.VMEM((S, C, W), bf16),
            dma((2 * tiles + 1,)),
            dma((S,)),
            dma((S,)),
            dma((2, half, QUARTERS)),
            dma((2, half, QUARTERS)),
            dma((QUARTERS, Z)),
            dma((QUARTERS, Z)),
            dma((QUARTERS, Z)),
            dma((QUARTERS, Z)),
            dma((2, half, QUARTERS)),
            dma((2, half, QUARTERS)),
            dma((S,)),
            dma((S,)),
        ],
        compiler_params=pltpu.CompilerParams(
            collective_id=0, has_side_effects=True, vmem_limit_bytes=56 * 1024 * 1024
        ),
        name="routed_experts",
    )(normed, residual, routes.T, route_weights.T, gate_w, up_w, down_w)


def exchange_kernel(T, blocks_ref, out_ref, land, send_sem, recv_sem):
    s_me = lax.axis_index("sp")
    t_me = lax.axis_index("tp")
    barrier = pltpu.get_barrier_semaphore()
    for i in range(1, T):
        peer = (s_me, lax.rem(t_me + i, T))
        pl.semaphore_signal(barrier, inc=1, device_id=peer, device_id_type=MESH)
    pl.semaphore_wait(barrier, T - 1)
    copies = []
    for i in range(1, T):
        target = lax.rem(t_me + i, T)
        copies.append(
            pltpu.make_async_remote_copy(
                src_ref=blocks_ref.at[target],
                dst_ref=land.at[t_me],
                send_sem=send_sem.at[i],
                recv_sem=recv_sem.at[i],
                device_id=(s_me, target),
                device_id_type=MESH,
            )
        )
    for cp in copies:
        cp.start()
    land[t_me] = blocks_ref[t_me]
    for cp in copies:
        cp.wait()
    out_ref[...] = land[...]


def exchange(blocks):
    T = blocks.shape[0]
    vmem = pl.BlockSpec(memory_space=pltpu.VMEM)
    return pl.pallas_call(
        functools.partial(exchange_kernel, T),
        out_shape=jax.ShapeDtypeStruct(blocks.shape, blocks.dtype),
        in_specs=[vmem],
        out_specs=vmem,
        scratch_shapes=[
            pltpu.VMEM(blocks.shape, blocks.dtype),
            pltpu.SemaphoreType.DMA((T,)),
            pltpu.SemaphoreType.DMA((T,)),
        ],
        compiler_params=pltpu.CompilerParams(collective_id=1, has_side_effects=True),
        name="exchange",
    )(blocks)


class Link:
    def __init__(self):
        self.sent = []

    def copy(self, src, dst, send_sem, recv_sem, peer):
        return pltpu.make_async_remote_copy(
            src_ref=src,
            dst_ref=dst,
            send_sem=send_sem,
            recv_sem=recv_sem,
            device_id=peer,
            device_id_type=MESH,
        )

    def start(self, cp, cond=None):
        self.sent.append((cp, cond))
        if cond is None:
            cp.start()
        else:
            pl.when(cond)(cp.start)

    def drain(self):
        for cp, cond in self.sent:
            if cond is None:
                cp.wait_send()
            else:
                pl.when(cond)(cp.wait_send)


def fused_kernel(
    T,
    C,
    taps_n,
    H,
    value_hbm,
    vgate_hbm,
    taps_ref,
    gain_ref,
    bias_ref,
    routes_ref,
    weights_ref,
    egain_ref,
    stream_hbm,
    outw_hbm,
    gate_hbm,
    up_hbm,
    down_hbm,
    out_ref,
    value_ref,
    vgate_ref,
    stream_ref,
    gbuf,
    halo_out,
    halo_in,
    cbuf,
    land,
    outw,
    res,
    meta,
    cho,
    hi,
    lo,
    tok,
    sbuf,
    X,
    wg,
    wd,
    hid,
    mine,
    pout,
    pin,
    ret,
    tot,
    tout,
    tin,
    tmid,
    rin,
    w_sem,
    halo_sem,
    ex_send,
    ex_recv,
    meta_send,
    meta_recv,
    tz_send,
    tz_recv,
    pl_send,
    pl_recv,
    sx_send,
    sx_recv,
    sy_send,
    sy_recv,
    rt_send,
    rt_recv,
    zo_send,
    zo_recv,
    tm_recv,
    nr_send,
    nr_recv,
):
    f32, bf16 = jnp.float32, jnp.bfloat16
    s = lax.axis_index("sp")
    t = lax.axis_index("tp")
    z, c = t // 2, t % 2
    Z, J = T // 2, 4
    gy, gx = s // 2, s % 2
    W = out_ref.shape[1]
    tokens = out_ref.shape[0]
    F = wd.shape[0]
    tiles = F // 128
    ch, run = value_ref.shape
    rim = gbuf.shape[0] - run
    link = Link()

    def plane(j):
        return (lax.rem(gy + j // 2, 2) * 2 + lax.rem(gx + j % 2, 2), t)

    def at_z(zt):
        return (s, zt * 2 + c)

    sibling = (s, z * 2 + 1 - c)

    zp = [z, 1 + z % 2, 2 + z % 2 - 2 * (z // 2), 3 - 3 * (z % 2)]
    middle = (z >= 1) & (z <= Z - 2)

    early = [
        pltpu.make_async_copy(src, dst, w_sem.at[2 * tiles + 2 + i])
        for i, (src, dst) in enumerate(
            ((value_hbm, value_ref), (vgate_hbm, vgate_ref), (stream_hbm, stream_ref))
        )
    ]
    for cp in early:
        cp.start()
    outw_load = pltpu.make_async_copy(outw_hbm, outw, w_sem.at[2 * tiles + 1])
    outw_load.start()
    loads = []
    for j in range(tiles):
        for k, src in enumerate((gate_hbm, up_hbm)):
            loads.append(
                pltpu.make_async_copy(
                    src.at[0, :, pl.ds(j * 128, 128)],
                    wg.at[j, :, pl.ds(k * 128, 128)],
                    w_sem.at[2 * j + k],
                )
            )
    down_load = pltpu.make_async_copy(down_hbm.at[0], wd, w_sem.at[2 * tiles])
    for cp in loads:
        cp.start()
    down_load.start()

    barrier = pltpu.get_barrier_semaphore()
    peers = [plane(j) for j in range(1, J)] + [(s, lax.rem(t + i, T)) for i in range(1, T)]
    for peer in peers:
        pl.semaphore_signal(barrier, inc=1, device_id=peer, device_id_type=MESH)

    early[0].wait()
    early[1].wait()
    gated = (
        value_ref[...].astype(f32) * jax.nn.sigmoid(vgate_ref[...].astype(f32))
    ).astype(bf16)
    turned = gated.astype(f32).T
    gbuf[rim:, :] = turned
    halo_out[...] = turned[run - rim :, :].astype(bf16)
    meta[z, 0:2, 0:tokens] = routes_ref[...].astype(f32)
    meta[z, 2:4, 0:tokens] = weights_ref[...]

    pl.semaphore_wait(barrier, len(peers))

    S = J
    halo = link.copy(
        halo_out, halo_in, halo_sem.at[0], halo_sem.at[1], (lax.rem(s + 1, S), t)
    )
    link.start(halo, s < S - 1)

    def mz(i, zs):
        return link.copy(
            meta.at[z], meta.at[z], meta_send.at[i - 1], meta_recv.at[z], at_z(zs)
        )

    for i in range(1, Z):
        link.start(mz(i, lax.rem(z + i, Z)))

    def conv(b):
        acc = jnp.zeros((tokens, ch), f32)
        for j in range(taps_n):
            lead = rim - (taps_n - 1) + b * tokens + j
            acc = acc + taps_ref[j : j + 1, :] * gbuf[lead : lead + tokens, :]
        cbuf[b] = acc.astype(bf16)

    for b in range(1, T):
        conv(b)

    @pl.when(s > 0)
    def _():
        halo.wait_recv()
        gbuf[0:rim, :] = halo_in[...].astype(f32)

    @pl.when(s == 0)
    def _():
        gbuf[0:rim, :] = jnp.zeros((rim, ch), f32)

    conv(0)

    exchanges = []
    for i in range(1, T):
        target = lax.rem(t + i, T)
        cp = link.copy(
            cbuf.at[target], land.at[t], ex_send.at[i - 1], ex_recv.at[i - 1], (s, target)
        )
        link.start(cp)
        exchanges.append(cp)
    land[t] = cbuf[t]

    metas = [
        link.copy(
            meta.at[zp[p]], meta.at[zp[p]], meta_send.at[p - 1], meta_recv.at[zp[p]], at_z(zp[p])
        )
        for p in range(1, Z)
    ]

    row = lax.broadcasted_iota(jnp.int32, (J, tokens), 0)
    ids = (((gy + (row >> 1)) & 1) * 2 + ((gx + (row & 1)) & 1)).astype(f32)
    earlier = jnp.where(
        lax.broadcasted_iota(jnp.int32, (tokens, tokens), 0)
        < lax.broadcasted_iota(jnp.int32, (tokens, tokens), 1),
        1.0,
        0.0,
    ).astype(bf16)
    slot = lax.broadcasted_iota(jnp.int32, (C, tokens), 0).astype(f32)
    def matrices(p):
        if p > 0:
            metas[p - 1].wait_recv()
        m = meta[zp[p]]
        r0, r1 = m[0:1, :tokens], m[1:2, :tokens]
        w0, w1 = m[2:3, :tokens], m[3:4, :tokens]
        hit0, hit1 = r0 == ids, r1 == ids
        named = jnp.where(hit0 | hit1, 1.0, 0.0)
        row_w = jnp.where(hit0, w0, 0.0) + jnp.where(hit1, w1, 0.0)
        rank = jnp.dot(named.astype(bf16), earlier, preferred_element_type=f32)
        choose, weigh = [], []
        for j in range(J):
            pick = jnp.where(rank[j : j + 1, :] == slot, named[j : j + 1, :], 0.0)
            choose.append(pick)
            weigh.append(pick * row_w[j : j + 1, :])
        cho[p] = jnp.concatenate(choose, axis=0).astype(bf16)
        spread = jnp.concatenate(weigh, axis=0).T
        high = spread.astype(bf16)
        hi[p] = high
        lo[p] = (spread - high.astype(f32)).astype(bf16)

    matrices(0)

    for cp in exchanges:
        cp.wait_recv()
    whole = jnp.concatenate([land[i] for i in range(T)], axis=1).astype(f32)
    center = jnp.mean(whole, axis=1, keepdims=True)
    whole = whole - center
    var = jnp.mean(whole * whole, axis=1, keepdims=True)
    act = jax.nn.silu(
        whole * lax.rsqrt(var + epsilon) * gain_ref[...] + bias_ref[...]
    ).astype(bf16)
    outw_load.wait()
    early[2].wait()
    step = 512
    square = jnp.zeros((tokens, 1), f32)
    for n in range(W // step):
        cut = slice(n * step, (n + 1) * step)
        r = (
            stream_ref[:, cut].astype(f32)
            + jnp.dot(act, outw[:, cut], preferred_element_type=f32)
        ).astype(bf16)
        res[:, cut] = r
        rf = r.astype(f32)
        square = square + jnp.sum(rf * rf, axis=1, keepdims=True)
    scale = lax.rsqrt(square * (1.0 / W) + epsilon)
    for n in range(W // step):
        cut = slice(n * step, (n + 1) * step)
        tok[z, :, cut] = (res[:, cut].astype(f32) * scale * egain_ref[:, cut]).astype(bf16)

    R = pout.shape[0]
    span, part = W // H, W // R

    def half(h):
        return pl.ds(h * span, span)

    def sign(d):
        return 1 if d == 0 else -1

    def inside(v):
        return (v >= 0) & (v < Z)

    def tz(d, k, h, steps):
        block = lax.rem(z - sign(d) * steps + Z, Z)
        return link.copy(
            tok.at[block, :, half(h)],
            tok.at[block, :, half(h)],
            tz_send.at[d, k - 1, h],
            tz_recv.at[d, k - 1, h],
            at_z(lax.rem(z + sign(d) + Z, Z)),
        )

    def arrive(k, h):
        for d in (0, 1):
            sg = sign(d)
            pl.when(inside(z - sg * k))(tz(d, k, h, k).wait_recv)
            if k < Z - 1:
                link.start(tz(d, k + 1, h, k), inside(z - sg * k) & inside(z + sg))

    def pland(p, j, h):
        return link.copy(
            sbuf.at[p, j - 1, :, half(h)],
            X.at[p, j, 0, :, half(h)],
            pl_send.at[p, j - 1, h],
            pl_recv.at[p, j - 1, h],
            plane(j),
        )

    def sibx(p, j, h):
        return link.copy(
            X.at[p, j, 0, :, half(h)],
            X.at[p, j, 1, :, half(h)],
            sx_send.at[p, j, h],
            sx_recv.at[p, j, h],
            sibling,
        )

    def select(p, h):
        for n in range(span // step):
            cut = slice(h * span + n * step, h * span + (n + 1) * step)
            sel = jnp.dot(cho[p], tok[zp[p], :, cut], preferred_element_type=f32).astype(bf16)
            X[p, 0, 0, :, cut] = sel[0:C]
            for j in range(1, J):
                sbuf[p, j - 1, :, cut] = sel[j * C : (j + 1) * C]
        for j in (3, 1, 2):
            link.start(pland(p, j, h))
        link.start(sibx(p, 0, h))

    def forward(p, h):
        for j in (3, 1, 2):
            pland(p, j, h).wait_recv()
            link.start(sibx(p, j, h))

    def gather(p):
        for h in range(H):
            for j in range(J):
                sibx(p, j, h).wait_recv()

    M = J * 2 * C

    def ffn_up(p, start=0, stop=tiles):
        if p == 0 and start == 0:
            for cp in loads:
                cp.wait()
        for j in range(start, stop):
            x = X[p].reshape(M, W)
            both = jnp.dot(x, wg[j], preferred_element_type=f32)
            g, u = both[:, :128], both[:, 128:]
            hid[:, j * 128 : (j + 1) * 128] = (jax.nn.silu(g) * u).astype(bf16)

    def siby(p, h):
        return link.copy(
            pout.at[h, p], pin.at[h, p], sy_send.at[p, h], sy_recv.at[p, h], sibling
        )

    def ffn_down(p, h):
        if p == 0 and h == 0:
            down_load.wait()
        for n in range(part // step):
            cut = slice(n * step, (n + 1) * step)
            full = slice(h * part + n * step, h * part + (n + 1) * step)
            y = jnp.dot(hid[...], wd[:, full], preferred_element_type=f32).astype(bf16)
            y = y.reshape(J, 2, C, step)
            mine[h, p, :, :, cut] = y[:, 0]
            pout[h, p, :, :, cut] = y[:, 1]
        link.start(siby(p, h))

    def back(p, j, h):
        return link.copy(
            mine.at[h, p, j],
            ret.at[h, p, j],
            rt_send.at[p, j - 1, h],
            rt_recv.at[p, j - 1, h],
            plane(j),
        )

    def neighbour_rows(spot, h):
        return link.copy(
            mine.at[h, 1], rin.at[spot, h], nr_send.at[h], nr_recv.at[spot, h], at_z(zp[1])
        )

    def give(p, h):
        siby(p, h).wait_recv()
        total = mine[h, p].astype(f32) + pin[h, p].astype(f32)
        if p == 1:
            mine[h, 1] = total.astype(bf16)
            link.start(neighbour_rows(z // 2, h))
            return
        if p == 0:

            @pl.when(middle)
            def _():
                neighbour_rows(0, h).wait_recv()
                neighbour_rows(1, h).wait_recv()
                mine[h, 0] = (total + rin[0, h].astype(f32) + rin[1, h].astype(f32)).astype(bf16)

            @pl.when(jnp.logical_not(middle))
            def _():
                mine[h, 0] = total.astype(bf16)

        else:
            mine[h, p] = total.astype(bf16)
        ret[h, p, 0] = mine[h, p, 0]
        for j in (3, 1, 2):
            link.start(back(p, j, h))

    def zout(p, h):
        return link.copy(
            tout.at[h, p - 2], tin.at[h, z], zo_send.at[p - 2, h], zo_recv.at[z, h], at_z(zp[p])
        )

    def zin(p, h):
        return link.copy(
            tout.at[h, 0], tin.at[h, zp[p]], zo_send.at[0, h], zo_recv.at[zp[p], h], at_z(zp[p])
        )

    def zmid(h):
        return link.copy(
            tout.at[h, 1], tmid.at[h], zo_send.at[1, h], tm_recv.at[h], at_z(zp[1])
        )

    def mixed_part(p, h):
        for j in (3, 1, 2):
            back(p, j, h).wait_recv()
        got = ret[h, p].reshape(J * C, part)
        return jnp.dot(hi[p], got, preferred_element_type=f32) + jnp.dot(
            lo[p], got, preferred_element_type=f32
        )

    end = jnp.logical_not(middle)

    def combine(p, h):
        tout[h, p - 2] = mixed_part(p, h).astype(bf16)
        if p == 2:
            link.start(zout(2, h), end)
        else:
            link.start(zmid(h), end)
            link.start(zout(3, h), middle)

    def merge(h):
        @pl.when(middle)
        def _():
            zmid(h).wait_recv()
            tout[h, 0] = (tout[h, 0].astype(f32) + tmid[h].astype(f32)).astype(bf16)

        link.start(zout(2, h), middle)

    for h in range(H):
        for d in (0, 1):
            link.start(tz(d, 1, h, 0), inside(z + sign(d)))
    select(0, 0)
    select(0, 1)
    matrices(1)
    matrices(2)
    matrices(3)
    arrive(1, 0)
    select(1, 0)
    forward(0, 0)
    arrive(1, 1)
    select(1, 1)
    forward(0, 1)
    first, second = range(R // 2), range(R // 2, R)

    def each(f, p, pieces):
        for q in pieces:
            f(p, q)

    gather(0)
    ffn_up(0)
    arrive(2, 0)
    select(2, 0)
    forward(1, 0)
    each(ffn_down, 0, first)
    arrive(2, 1)
    select(2, 1)
    each(ffn_down, 0, second)
    forward(1, 1)
    gather(1)
    arrive(3, 0)
    select(3, 0)
    ffn_up(1)
    arrive(3, 1)
    select(3, 1)
    forward(2, 0)
    each(ffn_down, 1, first)
    forward(2, 1)
    each(ffn_down, 1, second)
    gather(2)
    each(give, 1, range(R))
    ffn_up(2)
    forward(3, 0)
    each(ffn_down, 2, first)
    forward(3, 1)
    each(ffn_down, 2, second)
    each(give, 2, first)
    gather(3)
    ffn_up(3, 0, tiles // 2)
    each(give, 2, second)
    ffn_up(3, tiles // 2, tiles)
    each(ffn_down, 3, range(R))
    each(give, 3, first)
    each(combine, 2, first)
    for q in first:
        give(3, R // 2 + q)
        combine(2, R // 2 + q)
    for q in range(R):
        combine(3, q)
        give(0, q)
    for q in range(R):
        merge(q)
        cut = slice(q * part, (q + 1) * part)
        tot[:, cut] = res[:, cut].astype(f32) + mixed_part(0, q)
    for q in range(R):
        cut = slice(q * part, (q + 1) * part)
        zin(2, q).wait_recv()
        acc = tot[:, cut] + tin[q, zp[2]].astype(f32)

        @pl.when(middle)
        def _():
            out_ref[:, cut] = acc.astype(bf16)

        @pl.when(end)
        def _():
            zin(1, q).wait_recv()
            out_ref[:, cut] = (acc + tin[q, zp[1]].astype(f32)).astype(bf16)

    link.drain()


def fused(
    conv_value, conv_gate, conv_taps, norm_gain, norm_bias, out_weight, stream,
    routes, route_weights, expert_gain, gate_w, up_w, down_w,
):
    T = lax.axis_size("tp")
    S, Z = lax.axis_size("sp"), T // 2
    tokens, W = stream.shape
    C = routes.shape[1] * tokens // S
    F = gate_w.shape[2]
    ch, run = conv_value.shape
    taps_n = conv_taps.shape[1]
    rim = -(-(taps_n - 1) // 16) * 16
    tiles = F // 128
    H, R = 2, 4
    part = W // R
    f32, bf16 = jnp.float32, jnp.bfloat16
    vmem = pl.BlockSpec(memory_space=pltpu.VMEM)
    hbm = pl.BlockSpec(memory_space=pl.ANY)
    dma = pltpu.SemaphoreType.DMA
    rows = (R, Z, S, C, part)
    return pl.pallas_call(
        functools.partial(fused_kernel, T, C, taps_n, H),
        out_shape=jax.ShapeDtypeStruct((tokens, W), bf16),
        in_specs=[hbm] * 2 + [vmem] * 6 + [hbm] * 5,
        out_specs=vmem,
        scratch_shapes=[
            pltpu.VMEM((ch, run), bf16),
            pltpu.VMEM((ch, run), bf16),
            pltpu.VMEM((tokens, W), bf16),
            pltpu.VMEM((rim + run, ch), f32),
            pltpu.VMEM((rim, ch), bf16),
            pltpu.VMEM((rim, ch), bf16),
            pltpu.VMEM((T, tokens, ch), bf16),
            pltpu.VMEM((T, tokens, ch), bf16),
            pltpu.VMEM(out_weight.shape, bf16),
            pltpu.VMEM((tokens, W), bf16),
            pltpu.VMEM((Z, 8, 128), f32),
            pltpu.VMEM((Z, S * C, tokens), bf16),
            pltpu.VMEM((Z, tokens, S * C), bf16),
            pltpu.VMEM((Z, tokens, S * C), bf16),
            pltpu.VMEM((Z, tokens, W), bf16),
            pltpu.VMEM((Z, S - 1, C, W), bf16),
            pltpu.VMEM((Z, S, 2, C, W), bf16),
            pltpu.VMEM((tiles, W, 256), bf16),
            pltpu.VMEM((F, W), bf16),
            pltpu.VMEM((S * 2 * C, F), bf16),
            pltpu.VMEM(rows, bf16),
            pltpu.VMEM(rows, bf16),
            pltpu.VMEM(rows, bf16),
            pltpu.VMEM(rows, bf16),
            pltpu.VMEM((tokens, W), f32),
            pltpu.VMEM((R, 2, tokens, part), bf16),
            pltpu.VMEM((R, Z, tokens, part), bf16),
            pltpu.VMEM((R, tokens, part), bf16),
            pltpu.VMEM((2, R, S, C, part), bf16),
            dma((2 * tiles + 5,)),
            dma((2,)),
            dma((T - 1,)),
            dma((T - 1,)),
            dma((Z - 1,)),
            dma((Z,)),
            dma((2, Z - 1, H)),
            dma((2, Z - 1, H)),
            dma((Z, S - 1, H)),
            dma((Z, S - 1, H)),
            dma((Z, S, H)),
            dma((Z, S, H)),
            dma((Z, R)),
            dma((Z, R)),
            dma((Z, S - 1, R)),
            dma((Z, S - 1, R)),
            dma((2, R)),
            dma((Z, R)),
            dma((R,)),
            dma((R,)),
            dma((2, R)),
        ],
        compiler_params=pltpu.CompilerParams(
            collective_id=2, has_side_effects=True, vmem_limit_bytes=60 * 1024 * 1024
        ),
        name="fused_block",
    )(
        conv_value, conv_gate, conv_taps.T, norm_gain.reshape(1, -1), norm_bias.reshape(1, -1),
        routes.T, route_weights.T, expert_gain.reshape(1, -1), stream,
        out_weight, gate_w, up_w, down_w,
    )


def per_device(
    conv_value,
    conv_gate,
    conv_taps,
    norm_gain,
    norm_bias,
    out_weight,
    stream,
    routes,
    route_weights,
    expert_gain,
    expert_gate,
    expert_up,
    expert_down,
):
    square_plane = lax.axis_size("sp") == 4 and lax.axis_size("tp") == 8
    if square_plane and expert_gate.shape[2] % 128 == 0 and conv_value.shape[0] % 128 == 0:
        return fused(
            conv_value, conv_gate, conv_taps, norm_gain, norm_bias, out_weight, stream,
            routes, route_weights, expert_gain, expert_gate, expert_up, expert_down,
        )
    f32 = jnp.float32
    local_ch = conv_value.shape[0]
    run_len = conv_value.shape[1]
    kernel_len = conv_taps.shape[1]
    gated_input = (conv_value.astype(f32) * jax.nn.sigmoid(conv_gate.astype(f32))).astype(
        jnp.bfloat16
    )
    left_rim = shifted(gated_input[:, run_len - (kernel_len - 1) :], "sp", 1)
    padded = jnp.concatenate([left_rim, gated_input], axis=1).astype(f32)
    conv_sum = jnp.zeros((local_ch, run_len), f32)
    for offset in range(kernel_len):
        conv_sum = (
            conv_sum + conv_taps[:, offset : offset + 1] * padded[:, offset : offset + run_len]
        )
    conv_out = conv_sum.astype(jnp.bfloat16)
    parts = lax.axis_size("tp")
    tok_rows = run_len // parts
    pieces = exchange(conv_out.T.reshape(parts, tok_rows, local_ch))
    whole_conv = pieces.transpose(1, 0, 2).reshape(tok_rows, parts * local_ch).astype(f32)
    center = jnp.mean(whole_conv, axis=1, keepdims=True)
    spread = jnp.mean((whole_conv - center) ** 2, axis=1, keepdims=True)
    scaled = (whole_conv - center) * lax.rsqrt(spread + epsilon) * norm_gain + norm_bias
    token_major = jax.nn.silu(scaled).astype(jnp.bfloat16)
    projected = jnp.dot(token_major, out_weight, preferred_element_type=f32)
    residual = (stream.astype(f32) + projected).astype(jnp.bfloat16)
    res_float = residual.astype(f32)
    normed = (
        res_float
        * lax.rsqrt(jnp.mean(res_float * res_float, axis=1, keepdims=True) + epsilon)
        * expert_gain
    ).astype(jnp.bfloat16)
    return routed_experts(
        normed, residual, routes, route_weights, expert_gate, expert_up, expert_down
    )


def solution(mesh):
    return jax.shard_map(
        per_device,
        mesh=mesh,
        in_specs=(
            P("tp", "sp"),
            P("tp", "sp"),
            P("tp", None),
            P(),
            P(),
            P(),
            P(("sp", "tp"), None),
            P(("sp", "tp"), None),
            P(("sp", "tp"), None),
            P(),
            P("sp", None, "tp"),
            P("sp", None, "tp"),
            P("sp", "tp", None),
        ),
        out_specs=P(("sp", "tp"), None),
        check_vma=False,
    )
```
